512 devices in a mesh: sp: 64 (over z, y), tp: 8 (over x, core).
Axes of the slice: x: 4, y: 4, z: 16, core: 2. Of those that a mesh axis runs over, the one named last changes fastest.
Arguments:
- latent: bfloat16 [49152, 2048], P(('sp', 'tp')), may hold values from -6 to 6
- condition: float32 [2048], P('sp'), may hold values from -6 to 6
- context_condition: float32 [2048], P('sp'), may hold values from -6 to 6
- context: bfloat16 [1024, 2048], P('sp'), may hold values from -6 to 6
- norm_gain: float32 [2048], replicated, may hold values from 0.1 to 1.9
- shift_weight: bfloat16 [2048, 2048], P('sp', 'tp'), may hold values from -0.375 to 0.375
- scale_weight: bfloat16 [2048, 2048], P('sp', 'tp'), may hold values from -0.375 to 0.375
- gate_weight: bfloat16 [2048, 2048], P('sp', 'tp'), may hold values from -0.375 to 0.375
- query_weight: bfloat16 [2048, 2048], P(None, 'tp'), may hold values from -2 to 2
- key_matrix: bfloat16 [2048, 1024], P(None, 'tp'), may hold values from -2 to 2
- value_matrix: bfloat16 [2048, 1024], P(None, 'tp'), may hold values from -0.125 to 0.125
- sink_logit_head: float32 [16], P('tp'), may hold values from 6 to 10
- out_weight: bfloat16 [2048, 2048], P('tp'), may hold values from -0.125 to 0.125
Outputs:
- updated: bfloat16 [49152, 2048], P(('sp', 'tp'))
The draws below stay inside these ranges and needn't reach their ends.
All inputs are finite; a program needn't handle non-finite values.
Results may differ from the reference program's by a relative error of at most 0.012.
The reference program's roundings to bfloat16 on the way count: a program that leaves them out, or rounds other values in their place, can miss the bound.
Values may be sent and summed in bfloat16 or wider, within the bound.
A program may use at most 64 MiB of HBM per device.

```python
import jax
import jax.numpy as jnp
from jax import lax

MODEL_DIM = 2048
QUERY_HEADS = 16
KEY_VALUE_HEADS = 8
HEAD_DIM = 128
WINDOW_REACH = 128
GRID_W = 64
CTX = 1024
TOKENS = 49152
N_TP = 8


def query_shared_group(key):
    return jax.random.normal(jax.random.fold_in(key, 101), (MODEL_DIM, QUERY_HEADS * HEAD_DIM), jnp.float32) * MODEL_DIM ** (-0.5)


def draw_query_weight(key, part):
    return query_shared_group(key).astype(jnp.bfloat16)


def draw_key_matrix(key, part):
    sampled_weights = jax.random.normal(jax.random.fold_in(key, 202), (MODEL_DIM, KEY_VALUE_HEADS * HEAD_DIM), jnp.float32) * MODEL_DIM ** (-0.5)
    return sampled_weights.astype(jnp.bfloat16)


def raised(drawn, stream_key, source, target, shards_of, factor):
    owner, partner = [(jnp.arange(drawn.shape[dim]) // (drawn.shape[dim] // shards_of)).reshape([-1 if axis == dim else 1 for axis in range(drawn.ndim)]) for dim in (source, target)]
    chosen = jax.random.permutation(stream_key, shards_of)[partner]
    strong = (owner == chosen) | (owner == (partner + shards_of // 2) % shards_of)
    return jnp.where(strong, factor * drawn, drawn)


def level_of(stream_key, dims, cuts, low, top_value):
    def one(axis_at, parts):
        steps = jax.random.uniform(jax.random.fold_in(jax.random.fold_in(stream_key, 6), axis_at), (parts,), jnp.float32, low / len(cuts), top_value / len(cuts))
        return jnp.repeat(jnp.exp(steps), dims[axis_at] // parts).reshape((-1,) + (1,) * (len(dims) - axis_at - 1))

    gain = one(*cuts[0])
    for cut in cuts[1:]:
        gain = gain * one(*cut)
    return gain


def normal_values(key, dims, spread, most, cuts=(), kind=jnp.bfloat16):
    drawn = spread * jax.random.normal(key, dims, jnp.float32)
    if cuts:
        drawn = drawn * level_of(key, dims, cuts, -0.22, 0.18)
    return jnp.clip(drawn, -most, most).astype(kind)


def heavy_noise(stream_key, extent, scale, most, cuts, heavy, kind=jnp.bfloat16):
    values = scale * jax.random.normal(stream_key, extent, jnp.float32)
    if cuts:
        values = values * level_of(stream_key, extent, cuts, -0.22, 0.18)
    return jnp.clip(raised(values, jax.random.fold_in(stream_key, 3), *heavy), -most, most).astype(kind)


def setup_inputs(seed: int = 0) -> dict:
    key_list = jax.random.split(jax.random.key(seed), 14)
    latent = normal_values(key_list[0], (TOKENS, MODEL_DIM), 1.0, 6.0, ((0, 512),))
    condition = normal_values(key_list[1], (MODEL_DIM,), 1.0, 6.0, ((0, 64),), jnp.float32)
    context_condition = normal_values(key_list[2], (MODEL_DIM,), 1.0, 6.0, ((0, 64),), jnp.float32)
    context = normal_values(key_list[3], (CTX, MODEL_DIM), 1.0, 6.0, ((0, 64),))
    norm_gain = jnp.clip(1.0 + 0.18 * jax.random.normal(key_list[4], (MODEL_DIM,), jnp.float32), 0.1, 1.9)
    shift_weight = heavy_noise(key_list[5], (MODEL_DIM, MODEL_DIM), MODEL_DIM ** -0.5, 0.375, ((0, 64), (1, 8)), (0, 1, 64, 4.0))
    scale_weight = heavy_noise(key_list[6], (MODEL_DIM, MODEL_DIM), MODEL_DIM ** -0.5, 0.375, ((0, 64), (1, 8)), (0, 1, 64, 4.0))
    gate_weight = heavy_noise(key_list[7], (MODEL_DIM, MODEL_DIM), MODEL_DIM ** -0.5, 0.375, ((0, 64), (1, 8)), (0, 1, 64, 4.0))
    query_weight = draw_query_weight(jax.random.fold_in(key_list[13], 71), 0)
    key_matrix = draw_key_matrix(jax.random.fold_in(key_list[13], 71), 0)
    value_matrix = normal_values(key_list[10], (MODEL_DIM, KEY_VALUE_HEADS * HEAD_DIM), MODEL_DIM ** -0.5, 0.125, ((1, 8),))
    sink_logit_head = jnp.clip(6.0 + 4.0 * jax.random.uniform(key_list[11], (QUERY_HEADS,), jnp.float32) ** level_of(key_list[11], (QUERY_HEADS,), ((0, 8),), -0.2, 0.2), 6.0, 10.0)
    out_weight = normal_values(key_list[12], (QUERY_HEADS * HEAD_DIM, MODEL_DIM), (QUERY_HEADS * HEAD_DIM) ** -0.5, 0.125, ((0, 8),))
    return {"latent": latent, "condition": condition, "context_condition": context_condition, "context": context, "norm_gain": norm_gain, "shift_weight": shift_weight, "scale_weight": scale_weight, "gate_weight": gate_weight, "query_weight": query_weight, "key_matrix": key_matrix, "value_matrix": value_matrix, "sink_logit_head": sink_logit_head, "out_weight": out_weight}


NORM_EPS = 1e-05
MASKED_SCORE = -1e+30

def rotate(vectors, position):
    quarter = HEAD_DIM // 4
    grid_row = (position // GRID_W).astype(jnp.float32)
    grid_col = (position % GRID_W).astype(jnp.float32)
    inv_freq = 10000.0 ** (-jnp.arange(0, HEAD_DIM // 2, 2, dtype=jnp.float32) / (HEAD_DIM // 2))
    angles = jnp.concatenate([grid_row[:, None] * inv_freq, grid_col[:, None] * inv_freq], axis=-1)
    cosine_table = jnp.cos(angles).reshape(-1, 1, 2, quarter)
    sine_table = jnp.sin(angles).reshape(-1, 1, 2, quarter)
    pieces = vectors.reshape(vectors.shape[0], vectors.shape[1], 2, 2, quarter)
    first_half = pieces[..., 0, :]
    second_half = pieces[..., 1, :]
    turned = jnp.stack([first_half * cosine_table - second_half * sine_table, first_half * sine_table + second_half * cosine_table], axis=-2)
    return turned.reshape(vectors.shape)

def modulation(vector, weight):
    active = jax.nn.silu(vector).astype(jnp.bfloat16)
    return jnp.dot(active[None, :], weight, preferred_element_type=jnp.float32)[0]

def modulated_norm(rows_in, norm_gain, shift, scale):
    floats = rows_in.astype(jnp.float32)
    normed = floats * lax.rsqrt(lax.optimization_barrier(jnp.mean(floats * floats, axis=-1, keepdims=True)) + NORM_EPS) * norm_gain
    return (normed * (1.0 + scale) + shift).astype(jnp.bfloat16)

def attend(queries, joined_keys, joined_values, context_key_rows, context_value_rows, sink_logit_head):
    latent_token_count = queries.shape[0]
    blocks = latent_token_count // WINDOW_REACH
    queries_per_group = QUERY_HEADS // KEY_VALUE_HEADS
    padding = ((WINDOW_REACH, WINDOW_REACH), (0, 0), (0, 0))
    keys_pad = jnp.pad(joined_keys, padding)
    values_pad = jnp.pad(joined_values, padding)
    ctx_key_f = context_key_rows.astype(jnp.float32)
    ctx_value_f = context_value_rows.astype(jnp.float32)
    factor = HEAD_DIM ** (-0.5)
    sink_logit_rows = sink_logit_head.reshape(KEY_VALUE_HEADS, queries_per_group, 1, 1)

    def one_block(block_index):
        begin_row = block_index * WINDOW_REACH
        query_row_block = lax.dynamic_slice_in_dim(queries, begin_row, WINDOW_REACH, 0)
        query_row_block = query_row_block.reshape(WINDOW_REACH, KEY_VALUE_HEADS, queries_per_group, HEAD_DIM).astype(jnp.float32)
        band_keys = lax.dynamic_slice_in_dim(keys_pad, begin_row, 3 * WINDOW_REACH, 0).astype(jnp.float32)
        band_values = lax.dynamic_slice_in_dim(values_pad, begin_row, 3 * WINDOW_REACH, 0).astype(jnp.float32)
        band_scores = jnp.einsum('qhgd,khd->hgqk', query_row_block, band_keys) * factor
        query_pos = begin_row + jnp.arange(WINDOW_REACH, dtype=jnp.int32)[:, None]
        key_pos = begin_row - WINDOW_REACH + jnp.arange(3 * WINDOW_REACH, dtype=jnp.int32)[None, :]
        allowed = (jnp.abs(key_pos - query_pos) <= WINDOW_REACH) & (key_pos >= 0) & (key_pos < latent_token_count)
        band_scores = jnp.where(allowed[None, None], band_scores, MASKED_SCORE)
        ctx_scores = jnp.einsum('qhgd,chd->hgqc', query_row_block, ctx_key_f) * factor
        maxima = jnp.maximum(jnp.maximum(lax.optimization_barrier(jnp.max(band_scores, axis=-1, keepdims=True)), lax.optimization_barrier(jnp.max(ctx_scores, axis=-1, keepdims=True))), sink_logit_rows)
        band_exp = jnp.exp(band_scores - maxima)
        ctx_exp = jnp.exp(ctx_scores - maxima)
        denominator = lax.optimization_barrier(jnp.sum(band_exp, axis=-1, keepdims=True)) + lax.optimization_barrier(jnp.sum(ctx_exp, axis=-1, keepdims=True)) + jnp.exp(sink_logit_rows - maxima)
        band_weights = (band_exp / denominator).astype(jnp.bfloat16).astype(jnp.float32)
        ctx_weights = (ctx_exp / denominator).astype(jnp.bfloat16).astype(jnp.float32)
        summed = jnp.einsum('hgqk,khd->qhgd', band_weights, band_values) + jnp.einsum('hgqc,chd->qhgd', ctx_weights, ctx_value_f)
        return summed.astype(jnp.bfloat16).reshape(WINDOW_REACH, QUERY_HEADS * HEAD_DIM)
    blocks_out = lax.map(one_block, jnp.arange(blocks, dtype=jnp.int32))
    return blocks_out.reshape(latent_token_count, QUERY_HEADS * HEAD_DIM)

def reference(latent, condition, context_condition, context, norm_gain, shift_weight, scale_weight, gate_weight, query_weight, key_matrix, value_matrix, sink_logit_head, out_weight):
    shift = modulation(condition, shift_weight)
    scale = modulation(condition, scale_weight)
    gate = modulation(condition, gate_weight)
    ctx_shift = modulation(context_condition, shift_weight)
    ctx_scale = modulation(context_condition, scale_weight)
    hidden_state = modulated_norm(latent, norm_gain, shift, scale)
    ctx_hidden = modulated_norm(context, norm_gain, ctx_shift, ctx_scale)
    latent_token_count = latent.shape[0]
    position = jnp.arange(latent_token_count, dtype=jnp.int32)
    queries = jnp.dot(hidden_state, query_weight, preferred_element_type=jnp.float32).reshape(latent_token_count, QUERY_HEADS, HEAD_DIM)
    queries = rotate(queries, position).astype(jnp.bfloat16)
    joined_keys = jnp.dot(hidden_state, key_matrix, preferred_element_type=jnp.float32).reshape(latent_token_count, KEY_VALUE_HEADS, HEAD_DIM)
    joined_keys = rotate(joined_keys, position).astype(jnp.bfloat16)
    joined_values = jnp.dot(hidden_state, value_matrix, preferred_element_type=jnp.float32).astype(jnp.bfloat16)
    joined_values = joined_values.reshape(latent_token_count, KEY_VALUE_HEADS, HEAD_DIM)
    context_key_rows = jnp.dot(ctx_hidden, key_matrix, preferred_element_type=jnp.float32).astype(jnp.bfloat16)
    context_value_rows = jnp.dot(ctx_hidden, value_matrix, preferred_element_type=jnp.float32).astype(jnp.bfloat16)
    context_key_rows = context_key_rows.reshape(-1, KEY_VALUE_HEADS, HEAD_DIM)
    context_value_rows = context_value_rows.reshape(-1, KEY_VALUE_HEADS, HEAD_DIM)
    attended = attend(queries, joined_keys, joined_values, context_key_rows, context_value_rows, sink_logit_head)
    group_width = QUERY_HEADS * HEAD_DIM // N_TP
    mixed_sum = jnp.zeros((latent_token_count, latent.shape[1]), jnp.float32)
    for member in range(N_TP):
        partial_value = jnp.dot(attended[:, member * group_width:(member + 1) * group_width], out_weight[member * group_width:(member + 1) * group_width], preferred_element_type=jnp.float32)
        rounded = lax.optimization_barrier(partial_value.astype(jnp.bfloat16))
        mixed_sum = mixed_sum + rounded.astype(jnp.float32)
    return (latent.astype(jnp.float32) + gate * mixed_sum).astype(jnp.bfloat16)
```

```python
import functools

import jax
import jax.numpy as jnp
import numpy as np
from jax import lax
from jax.experimental import pallas as pl
from jax.experimental.pallas import tpu as pltpu
from jax.sharding import PartitionSpec as P

HEAD_DIM = 128
REACH = 128
GRID_W = 64
NORM_EPS = 1e-05
MASKED_SCORE = -1e30
LANES = 128
NY = 4
NX = 4
MESH = pl.DeviceIdType.MESH
F32 = jnp.float32
BF16 = jnp.bfloat16
LOG2E = 1.4426950408889634


def loop(low, high, f):
    def step(i, carry):
        f(i)
        return carry

    lax.fori_loop(low, high, step, 0)


def block_kernel(
    n_sp,
    n_tp,
    cond_hbm,
    ctx_cond_hbm,
    gain_hbm,
    sink_hbm,
    rot_row_hbm,
    rot_col_hbm,
    latent_hbm,
    context_hbm,
    shift_hbm,
    scale_hbm,
    gate_hbm,
    wq_hbm,
    wk_hbm,
    wv_hbm,
    wo_hbm,
    out_ref,
    cond,
    ctx_cond,
    gain,
    sink,
    rot_row,
    rot_col,
    cos,
    sin,
    context,
    shift_w,
    scale_w,
    gate_w,
    wq,
    wkv,
    wo,
    lat,
    y_in,
    z_in,
    full,
    mod,
    hidden,
    ctx_hidden,
    queries,
    kv,
    ctx_kv,
    att,
    give,
    pin,
    outx,
    relay_in,
    x_in,
    own_total,
    load_sem,
    y_send,
    y_recv,
    z_send,
    z_recv,
    tp_send,
    tp_recv,
    lat_send,
    lat_recv,
    ctx_send,
    ctx_recv,
    halo_send,
    halo_recv,
    give_send,
    give_recv,
    rel_send,
    rel_recv,
    xs_send,
    xs_recv,
):
    sp = lax.axis_index("sp")
    tp = lax.axis_index("tp")
    n_z = n_sp // NY
    z, y = sp // NY, lax.rem(sp, NY)
    x, core = tp // 2, lax.rem(tp, 2)
    other = 1 - core
    partner = 2 * x + other

    def at_x(dx, c):
        return 2 * lax.rem(x + dx, NX) + c

    slots, rows, width = lat.shape
    group_rows = rows * n_tp
    half = rows // 2
    columns = shift_w.shape[1]
    chunks = columns // LANES
    vecs = y_in.shape[1]
    ctx_rows = context.shape[0]
    has_next, has_last = sp < n_sp - 1, sp > 0

    barrier = pltpu.get_barrier_semaphore()

    def greet(**where):
        pl.semaphore_signal(barrier, inc=1, device_id=where, device_id_type=MESH)

    loop(1, n_z, lambda d: greet(sp=lax.rem(z + d, n_z) * NY + y))
    loop(1, n_tp, lambda d: greet(tp=lax.rem(tp + d, n_tp)))
    loop(1, NY, lambda d: greet(sp=z * NY + lax.rem(y + d, NY)))
    cross_next = has_next & (y == NY - 1)
    cross_last = has_last & (y == 0)

    @pl.when(cross_next)
    def _():
        greet(sp=lax.rem(sp + 1, n_sp))

    @pl.when(cross_last)
    def _():
        greet(sp=lax.rem(sp + n_sp - 1, n_sp))

    own_lat = lat.at[tp]
    loads = {}
    for i, (name, src, dst) in enumerate(
        [
            ("cond", cond_hbm, cond),
            ("ctx_cond", ctx_cond_hbm, ctx_cond),
            ("shift", shift_hbm, shift_w),
            ("scale", scale_hbm, scale_w),
            ("gate", gate_hbm, gate_w),
            ("lat", latent_hbm, own_lat),
            ("row", rot_row_hbm.at[sp], rot_row),
            ("col", rot_col_hbm, rot_col),
            ("gain", gain_hbm, gain),
            ("context", context_hbm, context),
            ("wk", wk_hbm, wkv.at[:, 0:HEAD_DIM]),
            ("wv", wv_hbm, wkv.at[:, HEAD_DIM : 2 * HEAD_DIM]),
            ("wq", wq_hbm, wq),
            ("wo", wo_hbm, wo),
            ("sink", sink_hbm, sink),
        ]
    ):
        loads[name] = pltpu.make_async_copy(src, dst, load_sem.at[i])
        loads[name].start()

    def rcopy(src, dst, ssem, rsem, **where):
        return pltpu.make_async_remote_copy(
            src_ref=src,
            dst_ref=dst,
            send_sem=ssem,
            recv_sem=rsem,
            device_id=where,
            device_id_type=MESH,
        )

    def silu(v):
        return v / (1.0 + jnp.exp(-v))

    loads["cond"].wait()
    loads["ctx_cond"].wait()
    depth = cond.shape[1]
    row_id = lax.broadcasted_iota(jnp.int32, (16, depth), 0)
    active = jnp.where(
        row_id == 0,
        jnp.broadcast_to(silu(cond[...]), (16, depth)),
        jnp.broadcast_to(silu(ctx_cond[...]), (16, depth)),
    ).astype(BF16)
    vector = 0
    for name, weight, count in (("shift", shift_w, 2), ("scale", scale_w, 2), ("gate", gate_w, 1)):
        loads[name].wait()
        product = jnp.dot(active, weight[...], preferred_element_type=F32)
        for v in range(count):
            for j in range(chunks):
                y_in[y, vector * chunks + j] = product[v : v + 1, j * LANES : (j + 1) * LANES]
            vector += 1

    loads["row"].wait()
    loads["col"].wait()
    for g in range(group_rows // GRID_W):
        cos[g * GRID_W : (g + 1) * GRID_W, :] = rot_row[g : g + 1, :] + rot_col[0:GRID_W, :]
        sin[g * GRID_W : (g + 1) * GRID_W, :] = (
            rot_row[16 + g : 17 + g, :] + rot_col[GRID_W : 2 * GRID_W, :]
        )
    loads["lat"].wait()

    pl.semaphore_wait(
        barrier,
        (n_z - 1)
        + (n_tp - 1)
        + (NY - 1)
        + cross_next.astype(jnp.int32)
        + cross_last.astype(jnp.int32),
    )

    def y_copy(d, mine):
        peer = lax.rem(y + d, NY)
        slot = y if mine else peer
        return rcopy(
            y_in.at[y], y_in.at[slot], y_send.at[peer], y_recv.at[slot], sp=z * NY + peer
        )

    for d in (2, 1, 3):
        y_copy(d, True).start()

    low, high = pl.ds(0, half), pl.ds(half, half)

    def lat_copy(slot, part, sem, to):
        piece = lat.at[slot, part]
        which = 0 if part is not high else 1
        return rcopy(piece, piece, lat_send.at[sem], lat_recv.at[slot, which], tp=to)

    whole = pl.ds(0, rows)
    xp, xm = at_x(1, core), at_x(3, core)
    far = at_x(2, core)
    lat_sends = [
        lat_copy(tp, low, 0, xp),
        lat_copy(tp, high, 1, xm),
        lat_copy(tp, high, 2, xp),
        lat_copy(tp, low, 3, xm),
        lat_copy(tp, low, 4, partner),
        lat_copy(tp, high, 5, partner),
    ]
    for copy in lat_sends:
        copy.start()

    def lat_arrival(slot, which):
        lat_copy(slot, low if which == 0 else high, 0, partner).wait_recv()

    loop(1, NY, lambda d: y_copy(d, False).wait_recv())
    z_in[z] = jnp.sum(y_in[...], axis=0)

    def z_copy(d, mine):
        peer = lax.rem(z + d, n_z)
        slot = z if mine else peer
        return rcopy(
            z_in.at[z], z_in.at[slot], z_send.at[peer], z_recv.at[slot], sp=peer * NY + y
        )

    def far_first(i):
        step = (i + 1) // 2
        return n_z // 2 + jnp.where(lax.rem(i, 2) == 1, step, -step)

    loop(0, n_z - 1, lambda i: z_copy(far_first(i), True).start())
    loop(1, n_z, lambda d: z_copy(d, False).wait_recv())
    full[tp] = jnp.sum(z_in[...], axis=0)

    def tp_copy(d, mine):
        peer = lax.rem(tp + d, n_tp)
        slot = tp if mine else peer
        return rcopy(full.at[tp], full.at[slot], tp_send.at[peer], tp_recv.at[slot], tp=peer)

    loop(1, n_tp, lambda d: tp_copy(d, True).start())

    lat_arrival(xm, 0)
    relay_a = lat_copy(xm, low, 6, xp)
    relay_a.start()
    lat_arrival(xp, 1)
    relay_b = lat_copy(xp, high, 7, xm)
    relay_b.start()
    lat_sends += [relay_a, relay_b]
    lat_arrival(xm, 1)
    lat_arrival(xp, 0)
    for i, slot in enumerate((xm, xp)):
        for j, part in enumerate((low, high)):
            copy = lat_copy(slot, part, 8 + 2 * i + j, partner)
            copy.start()
            lat_sends.append(copy)

    loop(1, n_tp, lambda d: tp_copy(d, False).wait_recv())
    for t in range(n_tp):
        for v in range(5):
            for j in range(chunks):
                column = t * columns + j * LANES
                mod[v : v + 1, column : column + LANES] = full[t, v * chunks + j]
    loads["gain"].wait()
    gains = gain[...]
    mod[2:3, :] = gains * (1.0 + mod[2:3, :])
    mod[3:4, :] = gains * (1.0 + mod[3:4, :])

    def normed(block, shift_row, scale_row):
        floats = block.astype(F32)
        inverse = lax.rsqrt(jnp.mean(floats * floats, axis=-1, keepdims=True) + NORM_EPS)
        return (
            floats * inverse * mod[scale_row : scale_row + 1, :] + mod[shift_row : shift_row + 1, :]
        ).astype(BF16)

    loads["context"].wait()
    loads["wk"].wait()
    loads["wv"].wait()
    ctx_hidden[...] = normed(context[...], 1, 3)
    ctx_kv[sp] = jnp.dot(ctx_hidden[...], wkv[...], preferred_element_type=F32).astype(BF16)

    def ctx_copy(slot, peer, sem):
        return rcopy(
            ctx_kv.at[slot], ctx_kv.at[slot], ctx_send.at[sem], ctx_recv.at[slot], sp=peer
        )

    def ctx_z(i):
        peer = lax.rem(z + far_first(i), n_z) * NY + y
        return ctx_copy(sp, peer, i)

    loop(0, n_z - 1, lambda i: ctx_z(i).start())

    def ctx_y(i, d):
        step = (i + 1) // 2
        slot = lax.rem(z + n_z + jnp.where(lax.rem(i, 2) == 1, step, -step), n_z) * NY + y
        return slot, ctx_copy(slot, z * NY + lax.rem(y + d, NY), n_z - 1 + 3 * i + d - 1)

    def relay_ctx(i):
        slot, _ = ctx_y(i, 1)

        @pl.when(i > 0)
        def _():
            ctx_copy(slot, sp, 0).wait_recv()

        for d in (2, 1, 3):
            ctx_y(i, d)[1].start()

    relay_ctx(jnp.int32(0))

    lane = lax.broadcasted_iota(jnp.int32, (2 * rows, HEAD_DIM), 1)
    quarter = HEAD_DIM // 4
    low_half = lax.rem(lane, 2 * quarter) < quarter
    strip = 32

    def turned(u, cosine, sine):
        swapped = jnp.where(
            low_half, pltpu.roll(u, HEAD_DIM - quarter, 1), pltpu.roll(u, quarter, 1)
        )
        return (u * cosine + swapped * sine).astype(BF16)

    def process(chip):
        def norm_strip(i):
            for c in range(2):
                at = pl.multiple_of(i * strip, strip)
                hidden[pl.ds(pl.multiple_of(c * rows + at, strip), strip), :] = normed(
                    lat[2 * chip + c, pl.ds(at, strip), :], 0, 2
                )

        loop(0, rows // strip, norm_strip)
        begin = pl.multiple_of(chip * 2 * rows, strip)
        here = pl.ds(begin, 2 * rows)
        kept = pl.ds(pl.multiple_of(begin + REACH, strip), 2 * rows)
        cosine, sine = cos[here, :], sin[here, :]
        pair = jnp.dot(hidden[...], wkv[...], preferred_element_type=F32)
        kv[kept, 0:HEAD_DIM] = turned(pair[:, 0:HEAD_DIM], cosine, sine)
        kv[kept, HEAD_DIM:] = pair[:, HEAD_DIM:].astype(BF16)
        q = jnp.dot(hidden[...], wq[...], preferred_element_type=F32)
        for h in range(2):
            cols = slice(h * HEAD_DIM, (h + 1) * HEAD_DIM)
            queries[here, cols] = turned(q[:, cols], cosine, sine)

    loads["wq"].wait()

    def stage(k):
        chip = lax.rem(x + jnp.where(k == 1, 3, jnp.where(k == 2, 1, k - jnp.where(k == 3, 1, 0))), NX)
        slot = 2 * chip + other

        @pl.when(k == 3)
        def _():
            mine = 2 * chip + core
            lat_arrival(mine, 0)
            lat_copy(mine, low, 12, partner).start()
            lat_arrival(mine, 1)
            lat_copy(mine, high, 13, partner).start()
            loop(3, 7, relay_ctx)

        lat_arrival(slot, 0)
        lat_arrival(slot, 1)
        process(chip)

        @pl.when(k == 2)
        def _():
            loop(1, 3, relay_ctx)

    loop(0, 4, stage)
    lat_sends += [lat_copy(far, low, 12, partner), lat_copy(far, high, 13, partner)]

    def halo_copy(up):
        source = group_rows if up else REACH
        target = 0 if up else group_rows + REACH
        which = 0 if up else 1
        return rcopy(
            kv.at[pl.ds(source, REACH)],
            kv.at[pl.ds(target, REACH)],
            halo_send.at[which],
            halo_recv.at[which],
            sp=lax.rem(sp + (1 if up else n_sp - 1), n_sp),
        )

    @pl.when(has_next)
    def _():
        halo_copy(True).start()

    @pl.when(has_last)
    def _():
        halo_copy(False).start()

    @pl.when(jnp.logical_not(has_last))
    def _():
        kv[0:REACH, :] = jnp.zeros((REACH, 2 * HEAD_DIM), BF16)

    @pl.when(jnp.logical_not(has_next))
    def _():
        kv[group_rows + REACH :, :] = jnp.zeros((REACH, 2 * HEAD_DIM), BF16)

    loop(7, n_z, relay_ctx)

    loads["wo"].wait()
    loads["sink"].wait()

    @pl.when(has_last)
    def _():
        halo_copy(True).wait_recv()

    @pl.when(has_next)
    def _():
        halo_copy(False).wait_recv()

    def quad_arrivals(i):
        for d in range(1, NY):
            ctx_copy(i * NY + lax.rem(y + d, NY), sp, 0).wait_recv()

    loop(0, n_z, quad_arrivals)

    span = rows + 2 * REACH
    total_rows = group_rows * n_sp
    ctx_total = n_sp * ctx_rows
    factor = HEAD_DIM ** (-0.5) * LOG2E
    contract = (((1,), (1,)), ((), ()))

    def attend(slot):
        begin = pl.multiple_of(slot * rows, strip)
        here = pl.ds(begin, rows)
        around = pl.ds(begin, span)
        query_at = lax.rem(lax.broadcasted_iota(jnp.int32, (2 * rows, span), 0), rows) + REACH
        key_at = lax.broadcasted_iota(jnp.int32, (2 * rows, span), 1)
        key_pos = sp * group_rows + begin - REACH + key_at
        allowed = (jnp.abs(key_at - query_at) <= REACH) & (key_pos >= 0) & (key_pos < total_rows)
        q = jnp.concatenate([queries[here, 0:HEAD_DIM], queries[here, HEAD_DIM:]], axis=0)
        band = lax.dot_general(q, kv[around, 0:HEAD_DIM], contract, preferred_element_type=F32)
        band = jnp.where(allowed, band * factor, MASKED_SCORE)
        ctx_keys = ctx_kv[:, :, 0:HEAD_DIM].reshape(ctx_total, HEAD_DIM)
        ctx_values = ctx_kv[:, :, HEAD_DIM:].reshape(ctx_total, HEAD_DIM)
        far_logits = lax.dot_general(q, ctx_keys, contract, preferred_element_type=F32) * factor
        sinks = jnp.concatenate(
            [jnp.broadcast_to(sink[0:1, i : i + 1] * LOG2E, (rows, 1)) for i in range(2)], axis=0
        )
        top = jnp.maximum(
            jnp.maximum(
                jnp.max(band, axis=-1, keepdims=True), jnp.max(far_logits, axis=-1, keepdims=True)
            ),
            sinks,
        )
        band_exp = jnp.exp2(band - top)
        far_exp = jnp.exp2(far_logits - top)
        total = (
            jnp.sum(band_exp, axis=-1, keepdims=True)
            + jnp.sum(far_exp, axis=-1, keepdims=True)
            + jnp.exp2(sinks - top)
        )
        mixed = jnp.dot(
            band_exp.astype(BF16), kv[around, HEAD_DIM:], preferred_element_type=F32
        ) + jnp.dot(far_exp.astype(BF16), ctx_values, preferred_element_type=F32)
        mixed = (mixed / total).astype(BF16)
        for h in range(2):
            att[:, h * HEAD_DIM : (h + 1) * HEAD_DIM] = mixed[h * rows : (h + 1) * rows]

    def chip_of(k):
        return lax.rem(
            x + jnp.where(k == 0, 2, jnp.where(k == 1, 1, jnp.where(k == 2, 3, 0))), NX
        )

    def give_copy(k):
        return rcopy(give.at[k], pin.at[k], give_send.at[k], give_recv.at[k], tp=partner)

    def relay_copy(up):
        part, i, to = (low, 0, xp) if up else (high, 1, xm)
        return rcopy(outx.at[0, part], relay_in.at[i], rel_send.at[i], rel_recv.at[i], tp=to)

    def x_copy(i):
        part = high if i in (0, 3) else low
        side = i // 2
        return rcopy(
            outx.at[1 + side, part],
            x_in.at[side, part],
            xs_send.at[i],
            xs_recv.at[i],
            tp=xm if side else xp,
        )

    n_tile = 512

    def project(store):
        for j in range(width // n_tile):
            cols = slice(j * n_tile, (j + 1) * n_tile)
            store(cols, jnp.dot(att[...], wo[:, cols], preferred_element_type=F32))

    def sub_block(j):
        keep = (j == 2) | (j == 4) | (j == 6) | (j == 7)
        k = jnp.where(
            keep, jnp.where(j == 7, 3, (j - 2) // 2), jnp.where(j == 0, 0, (j + 1) // 2)
        )
        attend(2 * chip_of(k) + jnp.where(keep, core, other))

        @pl.when(jnp.logical_not(keep))
        def _():
            def store(cols, value):
                give[k, :, cols] = value.astype(BF16)

            project(store)
            give_copy(k).start()

        @pl.when(keep)
        def _():
            give_copy(k).wait_recv()

        @pl.when(keep & (j < 7))
        def _():
            def store(cols, value):
                outx[k, :, cols] = (value + pin[k, :, cols].astype(F32)).astype(BF16)

            project(store)

        @pl.when(j == 2)
        def _():
            relay_copy(True).start()
            relay_copy(False).start()

        @pl.when(j == 4)
        def _():
            x_copy(0).start()

        @pl.when(j == 6)
        def _():
            x_copy(2).start()

        @pl.when(j == 7)
        def _():
            def store(cols, value):
                own_total[:, cols] = value + pin[3, :, cols].astype(F32)

            project(store)

    loop(0, 8, sub_block)

    for up, i in ((True, 1), (False, 3)):
        part, side = (low, 0) if up else (high, 1)
        relay_copy(up).wait_recv()
        for s in range(half // 16):
            at = pl.ds((0 if up else half) + 16 * s, 16)
            outx[1 + side, at, :] = (
                outx[1 + side, at, :].astype(F32)
                + relay_in[side, pl.ds(16 * s, 16), :].astype(F32)
            ).astype(BF16)
        x_copy(i).start()

    for i in range(4):
        x_copy(i).wait_recv()

    def finish(i):
        at = pl.ds(pl.multiple_of(i * strip, strip), strip)
        mixed = own_total[at, :] + x_in[0, at, :].astype(F32) + x_in[1, at, :].astype(F32)
        out_ref[at, :] = (lat[tp, at, :].astype(F32) + mod[4:5, :] * mixed).astype(BF16)

    loop(0, rows // strip, finish)

    loop(1, NY, lambda d: y_copy(d, True).wait_send())
    loop(1, n_z, lambda d: z_copy(d, True).wait_send())
    loop(1, n_tp, lambda d: tp_copy(d, True).wait_send())
    for copy in lat_sends:
        copy.wait_send()
    loop(0, n_z - 1, lambda i: ctx_z(i).wait_send())

    def ctx_drain(i):
        for d in range(1, NY):
            ctx_y(i, d)[1].wait_send()

    loop(0, n_z, ctx_drain)
    loop(0, 4, lambda k: give_copy(k).wait_send())
    for up in (True, False):
        relay_copy(up).wait_send()
    for i in range(4):
        x_copy(i).wait_send()

    @pl.when(has_next)
    def _():
        halo_copy(True).wait_send()

    @pl.when(has_last)
    def _():
        halo_copy(False).wait_send()


def angle_tables(total_rows, n_sp):
    inv_freq = np.power(
        10000.0, -np.arange(0, HEAD_DIM // 2, 2, dtype=np.float64) / (HEAD_DIM // 2)
    ).astype(np.float32)

    def tables(count):
        angle = (np.arange(count, dtype=np.float32)[:, None] * inv_freq).astype(np.float64)
        cosine, sine = np.cos(angle), np.sin(angle)
        return (
            np.concatenate([cosine, cosine], axis=1).astype(np.float32),
            np.concatenate([-sine, sine], axis=1).astype(np.float32),
        )

    half = HEAD_DIM // 2
    grid_rows = total_rows // GRID_W
    per = grid_rows // n_sp
    by_row, by_col = tables(grid_rows), tables(GRID_W)
    rows = np.zeros((n_sp, 32, HEAD_DIM), np.float32)
    rows[:, 0:per, :half] = by_row[0].reshape(n_sp, per, half)
    rows[:, 16 : 16 + per, :half] = by_row[1].reshape(n_sp, per, half)
    cols = np.zeros((2 * GRID_W, HEAD_DIM), np.float32)
    cols[:GRID_W, half:] = by_col[0]
    cols[GRID_W:, half:] = by_col[1]
    return rows, cols


def shards(
    n_sp,
    n_tp,
    latent,
    condition,
    context_condition,
    context,
    norm_gain,
    shift_weight,
    scale_weight,
    gate_weight,
    query_weight,
    key_matrix,
    value_matrix,
    sink_logit_head,
    out_weight,
):
    rows, width = latent.shape
    group_rows = rows * n_tp
    rot_rows, rot_cols = angle_tables(group_rows * n_sp, n_sp)
    columns = shift_weight.shape[1]
    groups = 5 * columns // LANES
    query_width = query_weight.shape[1]
    ctx_rows = context.shape[0]
    n_z = n_sp // NY
    dma = pltpu.SemaphoreType.DMA
    vmem = pl.BlockSpec(memory_space=pltpu.VMEM)
    anywhere = pl.BlockSpec(memory_space=pl.ANY)
    half = rows // 2

    def like(array):
        return pltpu.VMEM(array.shape, array.dtype)

    condition = condition.reshape(1, -1)
    context_condition = context_condition.reshape(1, -1)
    norm_gain = norm_gain.reshape(1, -1)
    sink = sink_logit_head.reshape(1, -1)
    return pl.pallas_call(
        functools.partial(block_kernel, n_sp, n_tp),
        out_shape=jax.ShapeDtypeStruct((rows, width), BF16),
        in_specs=[anywhere] * 15,
        out_specs=vmem,
        scratch_shapes=[
            like(condition),
            like(context_condition),
            like(norm_gain),
            like(sink),
            pltpu.VMEM((32, HEAD_DIM), F32),
            pltpu.VMEM((2 * GRID_W, HEAD_DIM), F32),
            pltpu.VMEM((group_rows, HEAD_DIM), F32),
            pltpu.VMEM((group_rows, HEAD_DIM), F32),
            like(context),
            like(shift_weight),
            like(scale_weight),
            like(gate_weight),
            like(query_weight),
            pltpu.VMEM((width, 2 * HEAD_DIM), BF16),
            like(out_weight),
            pltpu.VMEM((n_tp, rows, width), BF16),
            pltpu.VMEM((NY, groups, 1, LANES), F32),
            pltpu.VMEM((n_z, groups, 1, LANES), F32),
            pltpu.VMEM((n_tp, groups, 1, LANES), F32),
            pltpu.VMEM((8, width), F32),
            pltpu.VMEM((2 * rows, width), BF16),
            like(context),
            pltpu.VMEM((group_rows, query_width), BF16),
            pltpu.VMEM((group_rows + 2 * REACH, 2 * HEAD_DIM), BF16),
            pltpu.VMEM((n_sp, ctx_rows, 2 * HEAD_DIM), BF16),
            pltpu.VMEM((rows, query_width), BF16),
            pltpu.VMEM((4, rows, width), BF16),
            pltpu.VMEM((4, rows, width), BF16),
            pltpu.VMEM((3, rows, width), BF16),
            pltpu.VMEM((2, half, width), BF16),
            pltpu.VMEM((2, rows, width), BF16),
            pltpu.VMEM((rows, width), F32),
            dma((15,)),
            dma((NY,)),
            dma((NY,)),
            dma((n_z,)),
            dma((n_z,)),
            dma((n_tp,)),
            dma((n_tp,)),
            dma((14,)),
            dma((n_tp, 2)),
            dma((n_z - 1 + 3 * n_z,)),
            dma((n_sp,)),
            dma((2,)),
            dma((2,)),
            dma((4,)),
            dma((4,)),
            dma((2,)),
            dma((2,)),
            dma((4,)),
            dma((4,)),
        ],
        compiler_params=pltpu.CompilerParams(
            collective_id=0, has_side_effects=True, vmem_limit_bytes=60 * 1024 * 1024
        ),
    )(
        condition,
        context_condition,
        norm_gain,
        sink,
        jnp.asarray(rot_rows),
        jnp.asarray(rot_cols),
        latent,
        context,
        shift_weight,
        scale_weight,
        gate_weight,
        query_weight,
        key_matrix,
        value_matrix,
        out_weight,
    )


def solution(mesh):
    placed = (
        P(("sp", "tp"), None),
        P("sp"),
        P("sp"),
        P("sp", None),
        P(),
        P("sp", "tp"),
        P("sp", "tp"),
        P("sp", "tp"),
        P(None, "tp"),
        P(None, "tp"),
        P(None, "tp"),
        P("tp"),
        P("tp", None),
    )
    return jax.shard_map(
        functools.partial(shards, mesh.shape["sp"], mesh.shape["tp"]),
        mesh=mesh,
        in_specs=placed,
        out_specs=P(("sp", "tp"), None),
        check_vma=False,
    )
```

```python
import functools

import jax
import jax.numpy as jnp
import numpy as np
from jax import lax
from jax.experimental import pallas as pl
from jax.experimental.pallas import tpu as pltpu
from jax.sharding import PartitionSpec as P

HEAD_DIM = 128
REACH = 128
GRID_W = 64
NORM_EPS = 1e-05
MASKED_SCORE = -1e30
LANES = 128
NY = 4
NX = 4
MESH = pl.DeviceIdType.MESH
F32 = jnp.float32
BF16 = jnp.bfloat16
LOG2E = 1.4426950408889634


def loop(low, high, f):
    def step(i, carry):
        f(i)
        return carry

    lax.fori_loop(low, high, step, 0)


def block_kernel(
    n_sp,
    n_tp,
    cond_hbm,
    ctx_cond_hbm,
    gain_hbm,
    sink_hbm,
    rot_row_hbm,
    rot_col_hbm,
    latent_hbm,
    context_hbm,
    shift_hbm,
    scale_hbm,
    gate_hbm,
    wq_hbm,
    wk_hbm,
    wv_hbm,
    wo_hbm,
    out_ref,
    cond,
    ctx_cond,
    gain,
    sink,
    rot_row,
    rot_col,
    cos,
    sin,
    context,
    shift_w,
    scale_w,
    gate_w,
    wq,
    wkv,
    wo,
    lat,
    z_in,
    full,
    inv,
    mod,
    hidden,
    ctx_hidden,
    queries,
    kv,
    ctx_kv,
    att,
    give,
    pin,
    outx,
    relay_in,
    x_in,
    kept,
    bias,
    load_sem,
    z_send,
    z_recv,
    xy_send,
    xy_recv,
    lat_send,
    lat_recv,
    ctx_send,
    ctx_recv,
    halo_send,
    halo_recv,
    give_send,
    give_recv,
    rel_send,
    rel_recv,
    xs_send,
    xs_recv,
):
    sp = lax.axis_index("sp")
    tp = lax.axis_index("tp")
    n_z = n_sp // NY
    z, x = sp // NY, tp // 2
    y, core = sp - NY * z, tp - 2 * x
    other = 1 - core
    partner = 2 * x + other

    def wrap(i, n):
        return jnp.where(i >= n, i - n, i)

    def at_x(dx, c):
        return 2 * wrap(x + dx, NX) + c

    slots, rows, width = lat.shape
    group_rows = rows * n_tp
    half = rows // 2
    columns = shift_w.shape[1]
    chunks = columns // LANES
    ctx_rows = context.shape[0]
    has_next, has_last = sp < n_sp - 1, sp > 0

    barrier = pltpu.get_barrier_semaphore()

    def greet(**where):
        pl.semaphore_signal(barrier, inc=1, device_id=where, device_id_type=MESH)

    zs = [wrap(z + d, n_z) for d in range(n_z)]
    ys = [wrap(y + d, NY) for d in range(NY)]
    tps = [wrap(tp + d, n_tp) for d in range(n_tp)]
    z_steps = (4, n_z - 4, 2, n_z - 2, 1, n_z - 1)
    for d in z_steps:
        greet(sp=zs[d] * NY + y)

    def plane(d):
        return z * NY + ys[d // n_tp], tps[d % n_tp]

    for d in range(1, NY * n_tp):
        to_sp, to_tp = plane(d)
        greet(sp=to_sp, tp=to_tp)
    cross_next = has_next & (y == NY - 1)
    cross_last = has_last & (y == 0)

    @pl.when(cross_next)
    def _():
        greet(sp=lax.rem(sp + 1, n_sp))

    @pl.when(cross_last)
    def _():
        greet(sp=lax.rem(sp + n_sp - 1, n_sp))

    own_lat = lat.at[tp]
    loads = {}
    for i, (name, src, dst) in enumerate(
        [
            ("cond", cond_hbm, cond),
            ("ctx_cond", ctx_cond_hbm, ctx_cond),
            ("shift", shift_hbm, shift_w),
            ("scale", scale_hbm, scale_w),
            ("gate", gate_hbm, gate_w),
            ("lat", latent_hbm, own_lat),
            ("row", rot_row_hbm.at[sp], rot_row),
            ("col", rot_col_hbm, rot_col),
            ("gain", gain_hbm, gain),
            ("context", context_hbm, context),
            ("wk", wk_hbm, wkv.at[:, 0:HEAD_DIM]),
            ("wv", wv_hbm, wkv.at[:, HEAD_DIM : 2 * HEAD_DIM]),
            ("wq", wq_hbm, wq),
            ("wo", wo_hbm, wo),
            ("sink", sink_hbm, sink),
        ]
    ):
        loads[name] = pltpu.make_async_copy(src, dst, load_sem.at[i])
        loads[name].start()

    def rcopy(src, dst, ssem, rsem, **where):
        return pltpu.make_async_remote_copy(
            src_ref=src,
            dst_ref=dst,
            send_sem=ssem,
            recv_sem=rsem,
            device_id=where,
            device_id_type=MESH,
        )

    def silu(v):
        return v / (1.0 + jnp.exp(-v))

    loads["cond"].wait()
    loads["ctx_cond"].wait()
    depth = cond.shape[1]
    row_id = lax.broadcasted_iota(jnp.int32, (16, depth), 0)
    active = jnp.where(
        row_id == 0,
        jnp.broadcast_to(silu(cond[...]), (16, depth)),
        jnp.broadcast_to(silu(ctx_cond[...]), (16, depth)),
    ).astype(BF16)
    vector = 0
    for name, weight, count in (("shift", shift_w, 2), ("scale", scale_w, 2), ("gate", gate_w, 1)):
        loads[name].wait()
        product = jnp.dot(active, weight[...], preferred_element_type=F32)
        for v in range(count):
            for j in range(chunks):
                z_in[0, vector * chunks + j] = product[v : v + 1, j * LANES : (j + 1) * LANES]
            vector += 1

    loads["row"].wait()
    loads["col"].wait()
    for g in range(group_rows // GRID_W):
        cos[g * GRID_W : (g + 1) * GRID_W, :] = rot_row[g : g + 1, :] + rot_col[0:GRID_W, :]
        sin[g * GRID_W : (g + 1) * GRID_W, :] = (
            rot_row[16 + g : 17 + g, :] + rot_col[GRID_W : 2 * GRID_W, :]
        )
    def mask_rows(i):
        at = pl.ds(pl.multiple_of(i * 64, 64), 64)
        shape = (64, 4 * rows)
        lane_at = lax.rem(lax.broadcasted_iota(jnp.int32, shape, 1), 2 * rows)
        row = lane_at + jnp.where(lane_at < rows, other * rows, (core - 1) * rows)
        key = lax.broadcasted_iota(jnp.int32, shape, 0) + i * 64
        bias[at, :] = jnp.where(jnp.abs(key - row - REACH) <= REACH, 0.0, MASKED_SCORE)

    loop(0, (2 * rows + 2 * REACH) // 64, mask_rows)
    loads["lat"].wait()

    pl.semaphore_wait(
        barrier,
        len(z_steps)
        + (NY * n_tp - 1)
        + cross_next.astype(jnp.int32)
        + cross_last.astype(jnp.int32),
    )

    def z_copy(source, slot, step, stage):
        return rcopy(
            z_in.at[source],
            z_in.at[slot],
            z_send.at[0],
            z_recv.at[stage],
            sp=zs[step] * NY + y,
        )

    def z_wait(stage, count):
        got = z_in.at[pl.ds(0, count)]
        rcopy(got, got, z_send.at[0], z_recv.at[stage], sp=sp).wait_recv()

    z_copy(0, 3, n_z - 2, 0).start()
    z_copy(0, 1, 1, 0).start()
    z_copy(0, 2, n_z - 1, 0).start()

    low, high = pl.ds(0, half), pl.ds(half, half)

    def lat_copy(slot, part, sem, to):
        piece = lat.at[slot, part]
        which = 0 if part is not high else 1
        return rcopy(piece, piece, lat_send.at[0], lat_recv.at[slot, which], tp=to)

    whole = pl.ds(0, rows)
    xp, xm = at_x(1, core), at_x(3, core)
    far = at_x(2, core)
    for copy in (
        lat_copy(tp, low, 0, xp),
        lat_copy(tp, high, 1, xm),
        lat_copy(tp, low, 4, partner),
        lat_copy(tp, high, 5, partner),
    ):
        copy.start()

    def lat_arrival(slot, which):
        lat_copy(slot, low if which == 0 else high, 0, partner).wait_recv()

    def invert(slot):
        floats = lat[slot].astype(F32)
        mean = jnp.mean(floats * floats, axis=-1, keepdims=True)
        inv[slot] = jnp.broadcast_to(lax.rsqrt(mean + NORM_EPS), (rows, LANES))

    z_wait(0, 3)
    z_in[4] = (z_in[0] + z_in[1]) + (z_in[2] + z_in[3])
    z_copy(4, 5, 2, 1).start()
    z_copy(4, 6, n_z - 2, 1).start()
    invert(tp)
    z_wait(1, 2)
    z_in[7] = z_in[5] + z_in[6]
    z_copy(7, 8, 4, 2).start()
    z_copy(7, 9, n_z - 4, 2).start()
    lat_arrival(partner, 0)
    lat_arrival(partner, 1)
    invert(partner)
    z_wait(2, 2)
    own_full = y * n_tp + tp
    full[own_full] = z_in[8] + z_in[9]

    def xy_copy(d, mine):
        to_sp, to_tp = plane(d)
        peer = ys[d // n_tp] * n_tp + to_tp
        slot = own_full if mine else peer
        return rcopy(
            full.at[own_full],
            full.at[slot],
            xy_send.at[0],
            xy_recv.at[0],
            sp=to_sp,
            tp=to_tp,
        )

    for d in range(1, NY * n_tp):
        xy_copy(d, True).start()

    for part, i, to in ((high, 2, xp), (low, 3, xm)):
        copy = lat_copy(tp, part, i, to)
        copy.start()

    for i, slot, order in ((0, xm, (0,)), (1, xp, (1,))):
        for j in order:
            part = (low, high)[j]
            lat_arrival(slot, j)
            copy = lat_copy(slot, part, 8 + 2 * i + j, partner)
            copy.start()
    xy_all = full.at[pl.ds(0, NY * n_tp - 1)]
    xy_total = rcopy(xy_all, xy_all, xy_send.at[0], xy_recv.at[0], sp=sp)
    xy_total.wait_recv()
    for t in range(n_tp):
        sums = full[t]
        for r in range(1, NY):
            sums = sums + full[r * n_tp + t]
        for v in range(5):
            for j in range(chunks):
                column = t * columns + j * LANES
                mod[v : v + 1, column : column + LANES] = sums[v * chunks + j]
    loads["gain"].wait()
    gains = gain[...]
    mod[2:3, :] = gains * (1.0 + mod[2:3, :])
    mod[3:4, :] = gains * (1.0 + mod[3:4, :])

    def normed(block, shift_row, scale_row):
        floats = block.astype(F32)
        inverse = lax.rsqrt(jnp.mean(floats * floats, axis=-1, keepdims=True) + NORM_EPS)
        return (
            floats * inverse * mod[scale_row : scale_row + 1, :] + mod[shift_row : shift_row + 1, :]
        ).astype(BF16)

    loads["context"].wait()
    loads["wk"].wait()
    loads["wv"].wait()
    ctx_hidden[...] = normed(context[...], 1, 3)
    ctx_kv[sp] = jnp.dot(ctx_hidden[...], wkv[...], preferred_element_type=F32).astype(BF16)

    def ctx_copy(slot, peer, sem):
        return rcopy(
            ctx_kv.at[slot], ctx_kv.at[slot], ctx_send.at[0], ctx_recv.at[sem], sp=peer
        )

    def near_first(i):
        return i // 2 + 1 if i % 2 == 0 else n_z - i // 2 - 1

    def ctx_z(i):
        return ctx_copy(sp, zs[near_first(i)] * NY + y, z)

    for i in range(n_z - 1):
        ctx_z(i).start()

    relay_a = lat_copy(xm, low, 6, xp)
    relay_a.start()
    relay_b = lat_copy(xp, high, 7, xm)
    relay_b.start()

    def ctx_y(i, d):
        slot = (zs[near_first(i - 1)] if i else z) * NY + y
        return slot, ctx_copy(slot, z * NY + ys[d], n_z)

    def relay_ctx(first, last):
        for i in range(first, last):
            if i:
                of = zs[near_first(i - 1)]
                ctx_copy(of * NY + y, sp, of).wait_recv()
            for d in (2, 1, 3):
                ctx_y(i, d)[1].start()

    relay_ctx(0, 1)

    lane = lax.broadcasted_iota(jnp.int32, (2 * rows, HEAD_DIM), 1)
    quarter = HEAD_DIM // 4
    low_half = lax.rem(lane, 2 * quarter) < quarter
    strip = 32

    def turned(u, cosine, sine):
        swapped = jnp.where(
            low_half, pltpu.roll(u, HEAD_DIM - quarter, 1), pltpu.roll(u, quarter, 1)
        )
        return (u * cosine + swapped * sine).astype(BF16)

    def halo_copy(up):
        source = group_rows if up else REACH
        target = 0 if up else group_rows + REACH
        which = 0 if up else 1
        return rcopy(
            kv.at[pl.ds(source, REACH)],
            kv.at[pl.ds(target, REACH)],
            halo_send.at[which],
            halo_recv.at[which],
            sp=lax.rem(sp + (1 if up else n_sp - 1), n_sp),
        )

    def process(chip, relay_one, relay_two):

        def norm_strip(i):
            at = pl.ds(pl.multiple_of(i * strip, strip), strip)
            for c in range(2):
                inverse = inv[2 * chip + c, at, :]
                to = pl.ds(pl.multiple_of(c * rows + i * strip, strip), strip)
                for j in range(width // LANES):
                    cols = slice(j * LANES, (j + 1) * LANES)
                    hidden[to, cols] = (
                        lat[2 * chip + c, at, cols].astype(F32) * inverse * mod[2:3, cols]
                        + mod[0:1, cols]
                    ).astype(BF16)

        loop(0, rows // strip, norm_strip)
        relay_ctx(*relay_one)
        begin = pl.multiple_of(chip * 2 * rows, strip)
        here = pl.ds(begin, 2 * rows)
        kept = pl.ds(pl.multiple_of(begin + REACH, strip), 2 * rows)
        cosine, sine = cos[here, :], sin[here, :]
        pair = jnp.dot(hidden[...], wkv[...], preferred_element_type=F32)
        kv[kept, 0:HEAD_DIM] = turned(pair[:, 0:HEAD_DIM], cosine, sine)
        kv[kept, HEAD_DIM:] = pair[:, HEAD_DIM:].astype(BF16)
        q = jnp.dot(hidden[...], wq[...], preferred_element_type=F32)
        for h in range(2):
            cols = slice(h * HEAD_DIM, (h + 1) * HEAD_DIM)
            queries[here, cols] = turned(q[:, cols], cosine, sine)

        @pl.when(has_next & (chip == NX - 1))
        def _():
            halo_copy(True).start()

        @pl.when(has_last & (chip == 0))
        def _():
            halo_copy(False).start()

        relay_ctx(*relay_two)

    loads["wq"].wait()

    near = jnp.where(x < 2, NX - 1, 1)

    polls = [((0, 0), (0, 0)), ((1, 3), (3, 5)), ((5, 7), (7, 9)), ((0, 0), (0, 0))]
    for k in range(NX):
        step = (0, near, NX - near, 2)[k]
        chip = lax.rem(x + step, NX)
        slot = 2 * chip + other
        if k == 1:
            for i, neighbour, j in ((0, xm, 1), (1, xp, 0)):
                part = (low, high)[j]
                lat_arrival(neighbour, j)
                copy = lat_copy(neighbour, part, 8 + 2 * i + j, partner)
                copy.start()
            invert(xm)
            invert(xp)
        if k == 3:
            lat_arrival(far, 0)
            lat_copy(far, low, 12, partner).start()
            lat_arrival(far, 1)
            lat_copy(far, high, 13, partner).start()
            invert(far)
            relay_ctx(9, n_z)
        if k:
            lat_arrival(slot, 0)
            lat_arrival(slot, 1)
            invert(slot)
        process(chip, *polls[k])


    @pl.when(jnp.logical_not(has_last))
    def _():
        kv[0:REACH, :] = jnp.zeros((REACH, 2 * HEAD_DIM), BF16)

    @pl.when(jnp.logical_not(has_next))
    def _():
        kv[group_rows + REACH :, :] = jnp.zeros((REACH, 2 * HEAD_DIM), BF16)

    loads["wo"].wait()
    loads["sink"].wait()

    @pl.when(has_last)
    def _():
        halo_copy(True).wait_recv()

    @pl.when(has_next)
    def _():
        halo_copy(False).wait_recv()

    rest = ctx_kv.at[pl.ds(0, n_z * (NY - 1))]
    rcopy(rest, rest, ctx_send.at[0], ctx_recv.at[n_z], sp=sp).wait_recv()

    span = 2 * rows + 2 * REACH
    across = (((0,), (0,)), ((), ()))
    total_rows = group_rows * n_sp
    ctx_total = n_sp * ctx_rows
    factor = HEAD_DIM ** (-0.5) * LOG2E
    contract = (((1,), (1,)), ((), ()))

    both = 2 * rows
    lanes = 2 * both

    def attend(chip):
        begin = pl.multiple_of(chip * both, strip)
        around = pl.ds(begin, span)
        given = pl.ds(pl.multiple_of(begin + other * rows, strip), rows)
        kept_at = pl.ds(pl.multiple_of(begin + core * rows, strip), rows)
        q = jnp.concatenate(
            [
                queries[at, h * HEAD_DIM : (h + 1) * HEAD_DIM]
                for h in range(2)
                for at in (given, kept_at)
            ],
            axis=0,
        )
        key_pos = (
            sp * group_rows + begin - REACH + lax.broadcasted_iota(jnp.int32, (span, lanes), 0)
        )
        outside = (key_pos < 0) | (key_pos >= total_rows)
        band = lax.dot_general(kv[around, 0:HEAD_DIM], q, contract, preferred_element_type=F32)
        band = jnp.where(outside, MASKED_SCORE, band * factor + bias[...])
        ctx_keys = ctx_kv[:, :, 0:HEAD_DIM].reshape(ctx_total, HEAD_DIM)
        ctx_values = ctx_kv[:, :, HEAD_DIM:].reshape(ctx_total, HEAD_DIM)
        far_logits = lax.dot_general(ctx_keys, q, contract, preferred_element_type=F32) * factor
        sinks = jnp.concatenate(
            [jnp.broadcast_to(sink[0:1, i : i + 1] * LOG2E, (1, both)) for i in range(2)], axis=1
        )
        top = jnp.maximum(
            jnp.maximum(
                jnp.max(band, axis=0, keepdims=True), jnp.max(far_logits, axis=0, keepdims=True)
            ),
            sinks,
        )
        band_exp = jnp.exp2(band - top)
        far_exp = jnp.exp2(far_logits - top)
        total = (
            jnp.sum(band_exp, axis=0, keepdims=True)
            + jnp.sum(far_exp, axis=0, keepdims=True)
            + jnp.exp2(sinks - top)
        )
        mixed = lax.dot_general(
            kv[around, HEAD_DIM:], band_exp.astype(BF16), across, preferred_element_type=F32
        ) + lax.dot_general(
            ctx_values, far_exp.astype(BF16), across, preferred_element_type=F32
        )
        mixed = (mixed / total).T.astype(BF16)
        for h in range(2):
            att[:, h * HEAD_DIM : (h + 1) * HEAD_DIM] = mixed[h * both : (h + 1) * both]

    def chip_of(k):
        return lax.rem(
            x + jnp.where(k == 0, 2, jnp.where(k == 1, 1, jnp.where(k == 2, 3, 0))), NX
        )

    def give_copy(k):
        return rcopy(give.at[k], pin.at[k], give_send.at[0], give_recv.at[k], tp=partner)

    def relay_copy(up):
        part, i, to = (low, 0, xp) if up else (high, 1, xm)
        return rcopy(outx.at[0, part], relay_in.at[i], rel_send.at[0], rel_recv.at[i], tp=to)

    def x_copy(i):
        part = high if i in (0, 3) else low
        side = i // 2
        return rcopy(
            outx.at[1 + side, part],
            x_in.at[side, part],
            xs_send.at[0],
            xs_recv.at[0],
            tp=xm if side else xp,
        )

    n_tile = width

    def project(k):
        for first, store in ((0, "give"), (rows, "keep")):
            for j in range(width // n_tile):
                cols = slice(j * n_tile, (j + 1) * n_tile)
                value = jnp.dot(
                    att[first : first + rows, :], wo[:, cols], preferred_element_type=F32
                )
                if store == "give":
                    give[k, :, cols] = value.astype(BF16)
                else:
                    kept[:, cols] = value
            if store == "give":
                give_copy(k).start()

    def add_given(k, store):
        give_copy(k).wait_recv()

        def one(i):
            at = pl.ds(pl.multiple_of(i * strip, strip), strip)
            store(at, kept[at, :] + pin[k, at, :].astype(F32))

        loop(0, rows // strip, one)

    def chip_block(k):
        attend(chip_of(k))

        @pl.when(k > 0)
        def _():
            def store(at, value):
                outx[k - 1, at, :] = value.astype(BF16)

            add_given(k - 1, store)

        @pl.when(k == 1)
        def _():
            relay_copy(True).start()
            relay_copy(False).start()

        @pl.when(k == 2)
        def _():
            x_copy(0).start()

        @pl.when(k == 3)
        def _():
            x_copy(2).start()

        project(k)

    loop(0, NX, chip_block)

    for up, i in ((True, 1), (False, 3)):
        part, side = (low, 0) if up else (high, 1)
        relay_copy(up).wait_recv()
        for s in range(half // 16):
            at = pl.ds((0 if up else half) + 16 * s, 16)
            outx[1 + side, at, :] = (
                outx[1 + side, at, :].astype(F32)
                + relay_in[side, pl.ds(16 * s, 16), :].astype(F32)
            ).astype(BF16)
        x_copy(i).start()

    def own_store(at, value):
        kept[at, :] = value

    add_given(NX - 1, own_store)
    z_sent = z_in.at[pl.ds(0, 7)]
    rcopy(z_sent, z_sent, z_send.at[0], z_recv.at[0], sp=sp).wait_send()
    xy_total.wait_send()
    sent = lat.at[pl.ds(0, 7)]
    rcopy(sent, sent, lat_send.at[0], lat_recv.at[0, 0], sp=sp).wait_send()
    sent = ctx_kv.at[pl.ds(0, n_z * NY - 1)]
    rcopy(sent, sent, ctx_send.at[0], ctx_recv.at[0], sp=sp).wait_send()

    @pl.when(has_next)
    def _():
        halo_copy(True).wait_send()

    @pl.when(has_last)
    def _():
        halo_copy(False).wait_send()

    def whole_copy(ref, ssem, rsem):
        return rcopy(ref, ref, ssem, rsem, sp=sp)

    whole_copy(x_in, xs_send.at[0], xs_recv.at[0]).wait_recv()

    def finish(i):
        at = pl.ds(pl.multiple_of(i * strip, strip), strip)
        mixed = kept[at, :] + x_in[0, at, :].astype(F32) + x_in[1, at, :].astype(F32)
        out_ref[at, :] = (lat[tp, at, :].astype(F32) + mod[4:5, :] * mixed).astype(BF16)

    loop(0, rows // strip, finish)

    whole_copy(give, give_send.at[0], give_recv.at[0]).wait_send()
    whole_copy(outx.at[0], rel_send.at[0], rel_recv.at[0]).wait_send()
    whole_copy(outx.at[pl.ds(1, 2)], xs_send.at[0], xs_recv.at[0]).wait_send()


def angle_tables(total_rows, n_sp):
    inv_freq = np.power(
        10000.0, -np.arange(0, HEAD_DIM // 2, 2, dtype=np.float64) / (HEAD_DIM // 2)
    ).astype(np.float32)

    def tables(count):
        angle = (np.arange(count, dtype=np.float32)[:, None] * inv_freq).astype(np.float64)
        cosine, sine = np.cos(angle), np.sin(angle)
        return (
            np.concatenate([cosine, cosine], axis=1).astype(np.float32),
            np.concatenate([-sine, sine], axis=1).astype(np.float32),
        )

    half = HEAD_DIM // 2
    grid_rows = total_rows // GRID_W
    per = grid_rows // n_sp
    by_row, by_col = tables(grid_rows), tables(GRID_W)
    rows = np.zeros((n_sp, 32, HEAD_DIM), np.float32)
    rows[:, 0:per, :half] = by_row[0].reshape(n_sp, per, half)
    rows[:, 16 : 16 + per, :half] = by_row[1].reshape(n_sp, per, half)
    cols = np.zeros((2 * GRID_W, HEAD_DIM), np.float32)
    cols[:GRID_W, half:] = by_col[0]
    cols[GRID_W:, half:] = by_col[1]
    return rows, cols


def shards(
    n_sp,
    n_tp,
    latent,
    condition,
    context_condition,
    context,
    norm_gain,
    shift_weight,
    scale_weight,
    gate_weight,
    query_weight,
    key_matrix,
    value_matrix,
    sink_logit_head,
    out_weight,
):
    rows, width = latent.shape
    group_rows = rows * n_tp
    rot_rows, rot_cols = angle_tables(group_rows * n_sp, n_sp)
    columns = shift_weight.shape[1]
    groups = 5 * columns // LANES
    query_width = query_weight.shape[1]
    ctx_rows = context.shape[0]
    n_z = n_sp // NY
    dma = pltpu.SemaphoreType.DMA
    vmem = pl.BlockSpec(memory_space=pltpu.VMEM)
    anywhere = pl.BlockSpec(memory_space=pltpu.HBM)
    half = rows // 2

    def like(array):
        return pltpu.VMEM(array.shape, array.dtype)

    condition = condition.reshape(1, -1)
    context_condition = context_condition.reshape(1, -1)
    norm_gain = norm_gain.reshape(1, -1)
    sink = sink_logit_head.reshape(1, -1)
    return pl.pallas_call(
        functools.partial(block_kernel, n_sp, n_tp),
        out_shape=pltpu.VMEM((rows, width), BF16),
        in_specs=[anywhere] * 15,
        out_specs=vmem,
        scratch_shapes=[
            like(condition),
            like(context_condition),
            like(norm_gain),
            like(sink),
            pltpu.VMEM((32, HEAD_DIM), F32),
            pltpu.VMEM((2 * GRID_W, HEAD_DIM), F32),
            pltpu.VMEM((group_rows, HEAD_DIM), F32),
            pltpu.VMEM((group_rows, HEAD_DIM), F32),
            like(context),
            like(shift_weight),
            like(scale_weight),
            like(gate_weight),
            like(query_weight),
            pltpu.VMEM((width, 2 * HEAD_DIM), BF16),
            like(out_weight),
            pltpu.VMEM((n_tp, rows, width), BF16),
            pltpu.VMEM((10, groups, 1, LANES), F32),
            pltpu.VMEM((NY * n_tp, groups, 1, LANES), F32),
            pltpu.VMEM((n_tp, rows, LANES), F32),
            pltpu.VMEM((8, width), F32),
            pltpu.VMEM((2 * rows, width), BF16),
            like(context),
            pltpu.VMEM((group_rows, query_width), BF16),
            pltpu.VMEM((group_rows + 2 * REACH, 2 * HEAD_DIM), BF16),
            pltpu.VMEM((n_sp, ctx_rows, 2 * HEAD_DIM), BF16),
            pltpu.VMEM((2 * rows, query_width), BF16),
            pltpu.VMEM((4, rows, width), BF16),
            pltpu.VMEM((4, rows, width), BF16),
            pltpu.VMEM((3, rows, width), BF16),
            pltpu.VMEM((2, half, width), BF16),
            pltpu.VMEM((2, rows, width), BF16),
            pltpu.VMEM((rows, width), F32),
            pltpu.VMEM((2 * rows + 2 * REACH, 4 * rows), F32),
            dma((15,)),
            dma((1,)),
            dma((3,)),
            dma((1,)),
            dma((1,)),
            dma((1,)),
            dma((n_tp, 2)),
            dma((1,)),
            dma((n_z + 1,)),
            dma((2,)),
            dma((2,)),
            dma((1,)),
            dma((4,)),
            dma((1,)),
            dma((2,)),
            dma((1,)),
            dma((1,)),
        ],
        compiler_params=pltpu.CompilerParams(
            collective_id=0, has_side_effects=True, vmem_limit_bytes=int(60 * 1024 * 1024)
        ),
    )(
        condition,
        context_condition,
        norm_gain,
        sink,
        jnp.asarray(rot_rows),
        jnp.asarray(rot_cols),
        latent,
        context,
        shift_weight,
        scale_weight,
        gate_weight,
        query_weight,
        key_matrix,
        value_matrix,
        out_weight,
    )


def solution(mesh):
    placed = (
        P(("sp", "tp"), None),
        P("sp"),
        P("sp"),
        P("sp", None),
        P(),
        P("sp", "tp"),
        P("sp", "tp"),
        P("sp", "tp"),
        P(None, "tp"),
        P(None, "tp"),
        P(None, "tp"),
        P("tp"),
        P("tp", None),
    )
    return jax.shard_map(
        functools.partial(shards, mesh.shape["sp"], mesh.shape["tp"]),
        mesh=mesh,
        in_specs=placed,
        out_specs=P(("sp", "tp"), None),
        check_vma=False,
    )
```

```python
import functools

import jax
import jax.numpy as jnp
import numpy as np
from jax import lax
from jax.experimental import pallas as pl
from jax.experimental.pallas import tpu as pltpu
from jax.sharding import PartitionSpec as P

HEAD_DIM = 128
REACH = 128
GRID_W = 64
NORM_EPS = 1e-05
MASKED_SCORE = -1e30
LANES = 128
NY = 4
NX = 4
MESH = pl.DeviceIdType.MESH
F32 = jnp.float32
BF16 = jnp.bfloat16
LOG2E = 1.4426950408889634


def loop(low, high, f):
    def step(i, carry):
        f(i)
        return carry

    lax.fori_loop(low, high, step, 0)


def block_kernel(
    n_sp,
    n_tp,
    cond_hbm,
    ctx_cond_hbm,
    gain_hbm,
    sink_hbm,
    rot_row_hbm,
    rot_col_hbm,
    latent_hbm,
    context_hbm,
    shift_hbm,
    scale_hbm,
    gate_hbm,
    wq_hbm,
    wk_hbm,
    wv_hbm,
    wo_hbm,
    out_ref,
    cond,
    ctx_cond,
    gain,
    sink,
    rot_row,
    rot_col,
    cos,
    sin,
    context,
    shift_w,
    scale_w,
    gate_w,
    wq,
    wkv,
    wo,
    lat,
    z_in,
    full,
    inv,
    mod,
    hidden,
    ctx_hidden,
    queries,
    kv,
    ctx_kv,
    att,
    give,
    pin,
    outx,
    x_in,
    att_out,
    att_in,
    wo_far,
    kept,
    bias,
    edge,
    load_sem,
    z_send,
    z_recv,
    xy_send,
    xy_recv,
    lat_send,
    lat_recv,
    ctx_send,
    ctx_recv,
    halo_send,
    halo_recv,
    give_send,
    give_recv,
    xs_send,
    xs_recv,
    att_send,
    att_recv,
    wf_send,
    wf_recv,
):
    sp = lax.axis_index("sp")
    tp = lax.axis_index("tp")
    n_z = n_sp // NY
    z, x = sp // NY, tp // 2
    y, core = sp - NY * z, tp - 2 * x
    other = 1 - core
    partner = 2 * x + other

    def wrap(i, n):
        return jnp.where(i >= n, i - n, i)

    def at_x(dx, c):
        return 2 * wrap(x + dx, NX) + c

    slots, rows, width = lat.shape
    group_rows = rows * n_tp
    half = rows // 2
    columns = shift_w.shape[1]
    chunks = columns // LANES
    ctx_rows = context.shape[0]
    has_next, has_last = sp < n_sp - 1, sp > 0

    barrier = pltpu.get_barrier_semaphore()

    def greet(**where):
        pl.semaphore_signal(barrier, inc=1, device_id=where, device_id_type=MESH)

    zs = [wrap(z + d, n_z) for d in range(n_z)]
    ys = [wrap(y + d, NY) for d in range(NY)]
    tps = [wrap(tp + d, n_tp) for d in range(n_tp)]
    far_first = [
        n_z // 2 + ((i + 1) // 2 if i % 2 else -((i + 1) // 2)) for i in range(n_z - 1)
    ]
    for d in far_first:
        greet(sp=zs[d] * NY + y)

    def plane(d):
        return z * NY + ys[d // n_tp], tps[d % n_tp]

    for d in range(1, NY * n_tp):
        to_sp, to_tp = plane(d)
        greet(sp=to_sp, tp=to_tp)
    cross_next = has_next & (y == NY - 1)
    cross_last = has_last & (y == 0)

    @pl.when(cross_next)
    def _():
        greet(sp=lax.rem(sp + 1, n_sp))

    @pl.when(cross_last)
    def _():
        greet(sp=lax.rem(sp + n_sp - 1, n_sp))

    own_lat = lat.at[tp]
    loads = {}
    for i, (name, src, dst) in enumerate(
        [
            ("cond", cond_hbm, cond),
            ("ctx_cond", ctx_cond_hbm, ctx_cond),
            ("shift", shift_hbm, shift_w),
            ("scale", scale_hbm, scale_w),
            ("gate", gate_hbm, gate_w),
            ("lat", latent_hbm, own_lat),
            ("row", rot_row_hbm.at[sp], rot_row),
            ("col", rot_col_hbm, rot_col),
            ("gain", gain_hbm, gain),
            ("context", context_hbm, context),
            ("wk", wk_hbm, wkv.at[:, 0:HEAD_DIM]),
            ("wv", wv_hbm, wkv.at[:, HEAD_DIM : 2 * HEAD_DIM]),
            ("wq", wq_hbm, wq),
            ("wo", wo_hbm, wo),
            ("sink", sink_hbm, sink),
        ]
    ):
        loads[name] = pltpu.make_async_copy(src, dst, load_sem.at[i])
        loads[name].start()

    def rcopy(src, dst, ssem, rsem, **where):
        return pltpu.make_async_remote_copy(
            src_ref=src,
            dst_ref=dst,
            send_sem=ssem,
            recv_sem=rsem,
            device_id=where,
            device_id_type=MESH,
        )

    def silu(v):
        return v / (1.0 + jnp.exp(-v))

    loads["cond"].wait()
    loads["ctx_cond"].wait()
    depth = cond.shape[1]
    row_id = lax.broadcasted_iota(jnp.int32, (16, depth), 0)
    active = jnp.where(
        row_id == 0,
        jnp.broadcast_to(silu(cond[...]), (16, depth)),
        jnp.broadcast_to(silu(ctx_cond[...]), (16, depth)),
    ).astype(BF16)
    vector = 0
    for name, weight, count in (("shift", shift_w, 2), ("scale", scale_w, 2), ("gate", gate_w, 1)):
        loads[name].wait()
        product = jnp.dot(active, weight[...], preferred_element_type=F32)
        for v in range(count):
            for j in range(chunks):
                z_in[z, vector * chunks + j] = product[v : v + 1, j * LANES : (j + 1) * LANES]
            vector += 1

    loads["lat"].wait()

    pl.semaphore_wait(
        barrier,
        (n_z - 1)
        + (NY * n_tp - 1)
        + cross_next.astype(jnp.int32)
        + cross_last.astype(jnp.int32),
    )

    def z_copy(d, slot):
        return rcopy(
            z_in.at[z], z_in.at[slot], z_send.at[0], z_recv.at[0], sp=zs[d] * NY + y
        )

    for d in far_first:
        z_copy(d, z).start()

    low, high = pl.ds(0, half), pl.ds(half, half)

    def lat_copy(slot, part, sem, to):
        piece = lat.at[slot, part]
        which = 0 if part is not high else 1
        return rcopy(piece, piece, lat_send.at[0], lat_recv.at[slot, which], tp=to)

    whole = pl.ds(0, rows)
    xp, xm = at_x(1, core), at_x(3, core)
    far = at_x(2, core)
    for copy in (
        lat_copy(tp, low, 0, xp),
        lat_copy(tp, high, 1, xm),
        lat_copy(tp, low, 4, partner),
        lat_copy(tp, high, 5, partner),
    ):
        copy.start()

    def lat_arrival(slot, which):
        lat_copy(slot, low if which == 0 else high, 0, partner).wait_recv()

    def invert(slot):
        floats = lat[slot].astype(F32)
        mean = jnp.mean(floats * floats, axis=-1, keepdims=True)
        inv[slot] = jnp.broadcast_to(lax.rsqrt(mean + NORM_EPS), (rows, LANES))

    wo_part = wo.shape[0] // NY // 2

    def far_weights(source, to_sp, to_tp, piece, sem):
        at = pl.ds(pl.multiple_of((2 * y + piece) * wo_part, wo_part), wo_part)
        return rcopy(
            source.at[at], wo_far.at[at], wf_send.at[0], wf_recv.at[sem], sp=to_sp, tp=to_tp
        )

    def share_far_weights(piece):
        far_weights(wo, sp, far, piece, piece).wait_recv()
        for d in (2, 1, 3):
            far_weights(wo_far, z * NY + ys[d], tp, piece, 2 + piece).start()

    loads["wo"].wait()
    far_weights(wo, sp, far, 0, 0).start()

    def rotary_and_mask():
        loads["row"].wait()
        loads["col"].wait()
        for g in range(group_rows // GRID_W):
            cos[g * GRID_W : (g + 1) * GRID_W, :] = rot_row[g : g + 1, :] + rot_col[0:GRID_W, :]
            sin[g * GRID_W : (g + 1) * GRID_W, :] = (
                rot_row[16 + g : 17 + g, :] + rot_col[GRID_W : 2 * GRID_W, :]
            )
        def mask_rows(i):
            at = pl.ds(pl.multiple_of(i * 64, 64), 64)
            shape = (64, 4 * rows)
            lane_at = lax.rem(lax.broadcasted_iota(jnp.int32, shape, 1), 2 * rows)
            row = lane_at + jnp.where(lane_at < rows, other * rows, (core - 1) * rows)
            key = lax.broadcasted_iota(jnp.int32, shape, 0) + i * 64
            bias[at, :] = jnp.where(jnp.abs(key - row - REACH) <= REACH, 0.0, MASKED_SCORE)

        loop(0, (2 * rows + 2 * REACH) // 64, mask_rows)

    rotary_and_mask()
    invert(tp)
    lat_arrival(partner, 0)
    lat_arrival(partner, 1)
    invert(partner)
    z_all = z_in.at[pl.ds(0, n_z - 1)]
    z_total = rcopy(z_all, z_all, z_send.at[0], z_recv.at[0], sp=sp)
    z_total.wait_recv()
    own_full = y * n_tp + tp
    full[own_full] = jnp.sum(z_in[...], axis=0)

    def xy_copy(d, mine):
        to_sp, to_tp = plane(d)
        peer = ys[d // n_tp] * n_tp + to_tp
        slot = own_full if mine else peer
        return rcopy(
            full.at[own_full],
            full.at[slot],
            xy_send.at[0],
            xy_recv.at[0],
            sp=to_sp,
            tp=to_tp,
        )

    for d in range(1, NY * n_tp):
        xy_copy(d, True).start()

    for part, i, to in ((high, 2, xp), (low, 3, xm)):
        copy = lat_copy(tp, part, i, to)
        copy.start()

    far_weights(wo, sp, far, 1, 1).start()

    for i, slot, order in ((0, xm, (0,)), (1, xp, (1,))):
        for j in order:
            part = (low, high)[j]
            lat_arrival(slot, j)
            copy = lat_copy(slot, part, 8 + 2 * i + j, partner)
            copy.start()
    share_far_weights(0)
    xy_all = full.at[pl.ds(0, NY * n_tp - 1)]
    xy_total = rcopy(xy_all, xy_all, xy_send.at[0], xy_recv.at[0], sp=sp)
    xy_total.wait_recv()
    for t in range(n_tp):
        sums = full[t]
        for r in range(1, NY):
            sums = sums + full[r * n_tp + t]
        for v in range(5):
            for j in range(chunks):
                column = t * columns + j * LANES
                mod[v : v + 1, column : column + LANES] = sums[v * chunks + j]
    loads["gain"].wait()
    gains = gain[...]
    mod[2:3, :] = gains * (1.0 + mod[2:3, :])
    mod[3:4, :] = gains * (1.0 + mod[3:4, :])

    def normed(block, shift_row, scale_row):
        floats = block.astype(F32)
        inverse = lax.rsqrt(jnp.mean(floats * floats, axis=-1, keepdims=True) + NORM_EPS)
        return (
            floats * inverse * mod[scale_row : scale_row + 1, :] + mod[shift_row : shift_row + 1, :]
        ).astype(BF16)

    loads["context"].wait()
    loads["wk"].wait()
    loads["wv"].wait()
    ctx_hidden[...] = normed(context[...], 1, 3)
    ctx_kv[sp] = jnp.dot(ctx_hidden[...], wkv[...], preferred_element_type=F32).astype(BF16)

    def ctx_copy(slot, peer, sem):
        return rcopy(
            ctx_kv.at[slot], ctx_kv.at[slot], ctx_send.at[0], ctx_recv.at[sem], sp=peer
        )

    def near_first(i):
        return i // 2 + 1 if i % 2 == 0 else n_z - i // 2 - 1

    def ctx_z(i):
        return ctx_copy(sp, zs[near_first(i)] * NY + y, z)

    for i in range(n_z - 1):
        ctx_z(i).start()

    relay_a = lat_copy(xm, low, 6, xp)
    relay_a.start()
    relay_b = lat_copy(xp, high, 7, xm)
    relay_b.start()

    def ctx_y(i, d):
        slot = (zs[near_first(i - 1)] if i else z) * NY + y
        return slot, ctx_copy(slot, z * NY + ys[d], n_z)

    def relay_ctx(first, last):
        for i in range(first, last):
            if i:
                of = zs[near_first(i - 1)]
                ctx_copy(of * NY + y, sp, of).wait_recv()
            for d in (2, 1, 3):
                ctx_y(i, d)[1].start()

    relay_ctx(0, 1)

    lane = lax.broadcasted_iota(jnp.int32, (2 * rows, HEAD_DIM), 1)
    quarter = HEAD_DIM // 4
    low_half = lax.rem(lane, 2 * quarter) < quarter
    strip = 32

    def turned(u, cosine, sine):
        swapped = jnp.where(
            low_half, pltpu.roll(u, HEAD_DIM - quarter, 1), pltpu.roll(u, quarter, 1)
        )
        return (u * cosine + swapped * sine).astype(BF16)

    def halo_copy(up):
        source = group_rows if up else REACH
        target = 0 if up else group_rows + REACH
        which = 0 if up else 1
        return rcopy(
            kv.at[pl.ds(source, REACH)],
            kv.at[pl.ds(target, REACH)],
            halo_send.at[which],
            halo_recv.at[which],
            sp=lax.rem(sp + (1 if up else n_sp - 1), n_sp),
        )

    def process(chip, relay_one, relay_two):

        def norm_strip(i):
            at = pl.ds(pl.multiple_of(i * strip, strip), strip)
            for c in range(2):
                inverse = inv[2 * chip + c, at, :]
                to = pl.ds(pl.multiple_of(c * rows + i * strip, strip), strip)
                for j in range(width // LANES):
                    cols = slice(j * LANES, (j + 1) * LANES)
                    hidden[to, cols] = (
                        lat[2 * chip + c, at, cols].astype(F32) * inverse * mod[2:3, cols]
                        + mod[0:1, cols]
                    ).astype(BF16)

        loop(0, rows // strip, norm_strip)
        relay_ctx(*relay_one)
        begin = pl.multiple_of(chip * 2 * rows, strip)
        here = pl.ds(begin, 2 * rows)
        kept = pl.ds(pl.multiple_of(begin + REACH, strip), 2 * rows)
        cosine, sine = cos[here, :], sin[here, :]
        pair = jnp.dot(hidden[...], wkv[...], preferred_element_type=F32)
        kv[kept, 0:HEAD_DIM] = turned(pair[:, 0:HEAD_DIM], cosine, sine)
        kv[kept, HEAD_DIM:] = pair[:, HEAD_DIM:].astype(BF16)
        q = jnp.dot(hidden[...], wq[...], preferred_element_type=F32)
        for h in range(2):
            cols = slice(h * HEAD_DIM, (h + 1) * HEAD_DIM)
            queries[here, cols] = turned(q[:, cols], cosine, sine)

        @pl.when(has_next & (chip == NX - 1))
        def _():
            halo_copy(True).start()

        @pl.when(has_last & (chip == 0))
        def _():
            halo_copy(False).start()

        relay_ctx(*relay_two)

    loads["wq"].wait()

    near = jnp.where(x < 2, NX - 1, 1)

    polls = [((0, 0), (0, 0)), ((1, 3), (3, 5)), ((5, 7), (7, 9)), ((0, 0), (0, 0))]
    for k in range(NX):
        step = (0, near, NX - near, 2)[k]
        chip = lax.rem(x + step, NX)
        slot = 2 * chip + other
        if k == 1:
            for i, neighbour, j in ((0, xm, 1), (1, xp, 0)):
                part = (low, high)[j]
                lat_arrival(neighbour, j)
                copy = lat_copy(neighbour, part, 8 + 2 * i + j, partner)
                copy.start()
            invert(xm)
            invert(xp)
        if k == 3:
            lat_arrival(far, 0)
            lat_copy(far, low, 12, partner).start()
            lat_arrival(far, 1)
            lat_copy(far, high, 13, partner).start()
            invert(far)
            relay_ctx(9, n_z)
        if k:
            lat_arrival(slot, 0)
            lat_arrival(slot, 1)
            invert(slot)
        process(chip, *polls[k])


    @pl.when(jnp.logical_not(has_last))
    def _():
        kv[0:REACH, :] = jnp.zeros((REACH, 2 * HEAD_DIM), BF16)

    @pl.when(jnp.logical_not(has_next))
    def _():
        kv[group_rows + REACH :, :] = jnp.zeros((REACH, 2 * HEAD_DIM), BF16)

    loads["sink"].wait()

    @pl.when(has_last)
    def _():
        halo_copy(True).wait_recv()

    @pl.when(has_next)
    def _():
        halo_copy(False).wait_recv()

    rest = ctx_kv.at[pl.ds(0, n_z * (NY - 1))]
    rcopy(rest, rest, ctx_send.at[0], ctx_recv.at[n_z], sp=sp).wait_recv()

    share_far_weights(1)

    span = 2 * rows + 2 * REACH
    across = (((0,), (0,)), ((), ()))
    total_rows = group_rows * n_sp
    ctx_total = n_sp * ctx_rows
    factor = HEAD_DIM ** (-0.5) * LOG2E
    contract = (((1,), (1,)), ((), ()))

    both = 2 * rows
    lanes = 2 * both

    def attend(chip):
        begin = pl.multiple_of(chip * both, strip)
        around = pl.ds(begin, span)
        given = pl.ds(pl.multiple_of(begin + other * rows, strip), rows)
        kept_at = pl.ds(pl.multiple_of(begin + core * rows, strip), rows)
        q = jnp.concatenate(
            [
                queries[at, h * HEAD_DIM : (h + 1) * HEAD_DIM]
                for h in range(2)
                for at in (given, kept_at)
            ],
            axis=0,
        )
        key_pos = (
            sp * group_rows + begin - REACH + lax.broadcasted_iota(jnp.int32, (span, LANES), 0)
        )
        edge[...] = jnp.where((key_pos < 0) | (key_pos >= total_rows), MASKED_SCORE, 0.0)
        ctx_keys = ctx_kv[:, :, 0:HEAD_DIM].reshape(ctx_total, HEAD_DIM)
        ctx_values = ctx_kv[:, :, HEAD_DIM:].reshape(ctx_total, HEAD_DIM)
        band_keys, band_values = kv[around, 0:HEAD_DIM], kv[around, HEAD_DIM:]
        sinks = jnp.concatenate(
            [jnp.broadcast_to(sink[0:1, i : i + 1] * LOG2E, (1, both)) for i in range(2)], axis=1
        )
        groups = [slice(0, 2 * LANES), slice(2 * LANES, lanes)]
        logits = []
        for g in groups:
            logits.append(
                (
                    lax.dot_general(band_keys, q[g], contract, preferred_element_type=F32),
                    lax.dot_general(ctx_keys, q[g], contract, preferred_element_type=F32),
                )
            )
        mixed = []
        for g, (band, far_logits) in zip(groups, logits):
            wide = (g.stop - g.start) // LANES
            band = band * factor + bias[:, g] + jnp.concatenate([edge[...]] * wide, axis=1)
            far_logits = far_logits * factor
            top = jnp.maximum(
                jnp.maximum(
                    jnp.max(band, axis=0, keepdims=True),
                    jnp.max(far_logits, axis=0, keepdims=True),
                ),
                sinks[:, g],
            )
            band_exp = jnp.exp2(band - top)
            far_exp = jnp.exp2(far_logits - top)
            total = (
                jnp.sum(band_exp, axis=0, keepdims=True)
                + jnp.sum(far_exp, axis=0, keepdims=True)
                + jnp.exp2(sinks[:, g] - top)
            )
            summed = lax.dot_general(
                band_values, band_exp.astype(BF16), across, preferred_element_type=F32
            ) + lax.dot_general(
                ctx_values, far_exp.astype(BF16), across, preferred_element_type=F32
            )
            mixed.append((summed / total).T.astype(BF16))
        mixed = jnp.concatenate(mixed, axis=0)
        for h in range(2):
            att[:, h * HEAD_DIM : (h + 1) * HEAD_DIM] = mixed[h * both : (h + 1) * both]

    def chip_of(k):
        return lax.rem(
            x + jnp.where(k == 0, 2, jnp.where(k == 1, 1, jnp.where(k == 2, 3, 0))), NX
        )

    def give_copy(k):
        return rcopy(give.at[k], pin.at[k], give_send.at[0], give_recv.at[k], tp=partner)

    def x_copy(side):
        return rcopy(
            outx.at[side],
            x_in.at[side],
            xs_send.at[0],
            xs_recv.at[0],
            tp=xm if side else xp,
        )

    def att_copy():
        return rcopy(att_out, att_in, att_send.at[0], att_recv.at[0], tp=far)

    n_tile = 512

    def project(k, with_far):
        for j in range(width // n_tile):
            cols = slice(j * n_tile, (j + 1) * n_tile)
            value = jnp.dot(att[...], wo[:, cols], preferred_element_type=F32)
            if with_far:
                value = value + jnp.dot(
                    att_in[...], wo_far[:, cols], preferred_element_type=F32
                )
            give[k, :, cols] = value[0:rows].astype(BF16)
            kept[:, cols] = value[rows:]
        give_copy(k).start()

    def add_given(k, store):
        give_copy(k).wait_recv()

        def one(i):
            at = pl.ds(pl.multiple_of(i * strip, strip), strip)
            store(at, kept[at, :] + pin[k, at, :].astype(F32))

        loop(0, rows // strip, one)

    def chip_block(k):
        attend(chip_of(k))

        @pl.when(k == 0)
        def _():
            att_out[...] = att[...]
            att_copy().start()

        @pl.when(k >= 2)
        def _():
            def store(at, value):
                outx[k - 2, at, :] = value.astype(BF16)

            add_given(k - 2, store)

        @pl.when(k == 2)
        def _():
            x_copy(0).start()

        @pl.when(k == 3)
        def _():
            x_copy(1).start()

        @pl.when((k == 1) | (k == 2))
        def _():
            project(k - 1, False)


    loop(0, NX, chip_block)

    att_copy().wait_recv()
    shared = wo_far.at[pl.ds(0, (NY - 1) * wo_part)]
    for sem in (2, 3):
        rcopy(shared, shared, wf_send.at[0], wf_recv.at[sem], sp=sp).wait_recv()
    project(2, True)

    z_total.wait_send()
    xy_total.wait_send()
    sent = lat.at[pl.ds(0, 7)]
    rcopy(sent, sent, lat_send.at[0], lat_recv.at[0, 0], sp=sp).wait_send()
    sent = ctx_kv.at[pl.ds(0, n_z * NY - 1)]
    rcopy(sent, sent, ctx_send.at[0], ctx_recv.at[0], sp=sp).wait_send()

    @pl.when(has_next)
    def _():
        halo_copy(True).wait_send()

    @pl.when(has_last)
    def _():
        halo_copy(False).wait_send()

    def whole_copy(ref, ssem, rsem):
        return rcopy(ref, ref, ssem, rsem, sp=sp)

    def own_store(at, value):
        kept[at, :] = value

    add_given(2, own_store)
    whole_copy(x_in, xs_send.at[0], xs_recv.at[0]).wait_recv()

    def finish(i):
        at = pl.ds(pl.multiple_of(i * strip, strip), strip)
        mixed = kept[at, :] + x_in[0, at, :].astype(F32) + x_in[1, at, :].astype(F32)
        out_ref[at, :] = (lat[tp, at, :].astype(F32) + mod[4:5, :] * mixed).astype(BF16)

    loop(0, rows // strip, finish)

    whole_copy(give, give_send.at[0], give_recv.at[0]).wait_send()
    whole_copy(outx, xs_send.at[0], xs_recv.at[0]).wait_send()
    whole_copy(wo_far, wf_send.at[0], wf_recv.at[0]).wait_send()
    att_copy().wait_send()


def angle_tables(total_rows, n_sp):
    inv_freq = np.power(
        10000.0, -np.arange(0, HEAD_DIM // 2, 2, dtype=np.float64) / (HEAD_DIM // 2)
    ).astype(np.float32)

    def tables(count):
        angle = (np.arange(count, dtype=np.float32)[:, None] * inv_freq).astype(np.float64)
        cosine, sine = np.cos(angle), np.sin(angle)
        return (
            np.concatenate([cosine, cosine], axis=1).astype(np.float32),
            np.concatenate([-sine, sine], axis=1).astype(np.float32),
        )

    half = HEAD_DIM // 2
    grid_rows = total_rows // GRID_W
    per = grid_rows // n_sp
    by_row, by_col = tables(grid_rows), tables(GRID_W)
    rows = np.zeros((n_sp, 32, HEAD_DIM), np.float32)
    rows[:, 0:per, :half] = by_row[0].reshape(n_sp, per, half)
    rows[:, 16 : 16 + per, :half] = by_row[1].reshape(n_sp, per, half)
    cols = np.zeros((2 * GRID_W, HEAD_DIM), np.float32)
    cols[:GRID_W, half:] = by_col[0]
    cols[GRID_W:, half:] = by_col[1]
    return rows, cols


def shards(
    n_sp,
    n_tp,
    latent,
    condition,
    context_condition,
    context,
    norm_gain,
    shift_weight,
    scale_weight,
    gate_weight,
    query_weight,
    key_matrix,
    value_matrix,
    sink_logit_head,
    out_weight,
):
    rows, width = latent.shape
    group_rows = rows * n_tp
    rot_rows, rot_cols = angle_tables(group_rows * n_sp, n_sp)
    columns = shift_weight.shape[1]
    groups = 5 * columns // LANES
    query_width = query_weight.shape[1]
    ctx_rows = context.shape[0]
    n_z = n_sp // NY
    dma = pltpu.SemaphoreType.DMA
    vmem = pl.BlockSpec(memory_space=pltpu.VMEM)
    anywhere = pl.BlockSpec(memory_space=pltpu.HBM)
    def like(array):
        return pltpu.VMEM(array.shape, array.dtype)

    condition = condition.reshape(1, -1)
    context_condition = context_condition.reshape(1, -1)
    norm_gain = norm_gain.reshape(1, -1)
    sink = sink_logit_head.reshape(1, -1)
    return pl.pallas_call(
        functools.partial(block_kernel, n_sp, n_tp),
        out_shape=pltpu.VMEM((rows, width), BF16),
        in_specs=[anywhere] * 15,
        out_specs=vmem,
        scratch_shapes=[
            like(condition),
            like(context_condition),
            like(norm_gain),
            like(sink),
            pltpu.VMEM((32, HEAD_DIM), F32),
            pltpu.VMEM((2 * GRID_W, HEAD_DIM), F32),
            pltpu.VMEM((group_rows, HEAD_DIM), F32),
            pltpu.VMEM((group_rows, HEAD_DIM), F32),
            like(context),
            like(shift_weight),
            like(scale_weight),
            like(gate_weight),
            like(query_weight),
            pltpu.VMEM((width, 2 * HEAD_DIM), BF16),
            like(out_weight),
            pltpu.VMEM((n_tp, rows, width), BF16),
            pltpu.VMEM((n_z, groups, 1, LANES), F32),
            pltpu.VMEM((NY * n_tp, groups, 1, LANES), F32),
            pltpu.VMEM((n_tp, rows, LANES), F32),
            pltpu.VMEM((8, width), F32),
            pltpu.VMEM((2 * rows, width), BF16),
            like(context),
            pltpu.VMEM((group_rows, query_width), BF16),
            pltpu.VMEM((group_rows + 2 * REACH, 2 * HEAD_DIM), BF16),
            pltpu.VMEM((n_sp, ctx_rows, 2 * HEAD_DIM), BF16),
            pltpu.VMEM((2 * rows, query_width), BF16),
            pltpu.VMEM((3, rows, width), BF16),
            pltpu.VMEM((3, rows, width), BF16),
            pltpu.VMEM((2, rows, width), BF16),
            pltpu.VMEM((2, rows, width), BF16),
            pltpu.VMEM((2 * rows, query_width), BF16),
            pltpu.VMEM((2 * rows, query_width), BF16),
            like(out_weight),
            pltpu.VMEM((rows, width), F32),
            pltpu.VMEM((2 * rows + 2 * REACH, 4 * rows), F32),
            pltpu.VMEM((2 * rows + 2 * REACH, LANES), F32),
            dma((15,)),
            dma((1,)),
            dma((1,)),
            dma((1,)),
            dma((1,)),
            dma((1,)),
            dma((n_tp, 2)),
            dma((1,)),
            dma((n_z + 1,)),
            dma((2,)),
            dma((2,)),
            dma((1,)),
            dma((3,)),
            dma((1,)),
            dma((1,)),
            dma((1,)),
            dma((1,)),
            dma((1,)),
            dma((4,)),
        ],
        compiler_params=pltpu.CompilerParams(
            collective_id=0, has_side_effects=True, vmem_limit_bytes=int(60 * 1024 * 1024)
        ),
    )(
        condition,
        context_condition,
        norm_gain,
        sink,
        jnp.asarray(rot_rows),
        jnp.asarray(rot_cols),
        latent,
        context,
        shift_weight,
        scale_weight,
        gate_weight,
        query_weight,
        key_matrix,
        value_matrix,
        out_weight,
    )


def solution(mesh):
    placed = (
        P(("sp", "tp"), None),
        P("sp"),
        P("sp"),
        P("sp", None),
        P(),
        P("sp", "tp"),
        P("sp", "tp"),
        P("sp", "tp"),
        P(None, "tp"),
        P(None, "tp"),
        P(None, "tp"),
        P("tp"),
        P("tp", None),
    )
    return jax.shard_map(
        functools.partial(shards, mesh.shape["sp"], mesh.shape["tp"]),
        mesh=mesh,
        in_specs=placed,
        out_specs=P(("sp", "tp"), None),
        check_vma=False,
    )
```

```python
import functools

import jax
import jax.numpy as jnp
import numpy as np
from jax import lax
from jax.experimental import pallas as pl
from jax.experimental.pallas import tpu as pltpu
from jax.sharding import PartitionSpec as P

HEAD_DIM = 128
REACH = 128
GRID_W = 64
NORM_EPS = 1e-05
MASKED_SCORE = -1e30
LANES = 128
NY = 4
NX = 4
MESH = pl.DeviceIdType.MESH
F32 = jnp.float32
BF16 = jnp.bfloat16
LOG2E = 1.4426950408889634


def loop(low, high, f):
    def step(i, carry):
        f(i)
        return carry

    lax.fori_loop(low, high, step, 0)


def block_kernel(
    n_sp,
    n_tp,
    cond_hbm,
    ctx_cond_hbm,
    gain_hbm,
    sink_hbm,
    rot_row_hbm,
    rot_col_hbm,
    latent_hbm,
    context_hbm,
    shift_hbm,
    scale_hbm,
    gate_hbm,
    wq_hbm,
    wk_hbm,
    wv_hbm,
    wo_hbm,
    out_ref,
    cond,
    ctx_cond,
    gain,
    sink,
    rot_row,
    rot_col,
    cos,
    sin,
    context,
    shift_w,
    scale_w,
    gate_w,
    wq,
    wkv,
    wo,
    lat,
    z_in,
    full,
    inv,
    mod,
    hidden,
    ctx_hidden,
    queries,
    kv,
    ctx_kv,
    att,
    give,
    pin,
    outx,
    x_in,
    att_out,
    att_in,
    wo_far,
    kept,
    bias,
    edge,
    load_sem,
    z_send,
    z_recv,
    xy_send,
    xy_recv,
    lat_send,
    lat_recv,
    ctx_send,
    ctx_recv,
    halo_send,
    halo_recv,
    give_send,
    give_recv,
    xs_send,
    xs_recv,
    att_send,
    att_recv,
    wf_send,
    wf_recv,
):
    sp = lax.axis_index("sp")
    tp = lax.axis_index("tp")
    n_z = n_sp // NY
    z, x = sp // NY, tp // 2
    y, core = sp - NY * z, tp - 2 * x
    other = 1 - core
    partner = 2 * x + other

    def wrap(i, n):
        return jnp.where(i >= n, i - n, i)

    def at_x(dx, c):
        return 2 * wrap(x + dx, NX) + c

    slots, rows, width = lat.shape
    group_rows = rows * n_tp
    half = rows // 2
    columns = shift_w.shape[1]
    chunks = columns // LANES
    ctx_rows = context.shape[0]
    has_next, has_last = sp < n_sp - 1, sp > 0

    barrier = pltpu.get_barrier_semaphore()

    def greet(**where):
        pl.semaphore_signal(barrier, inc=1, device_id=where, device_id_type=MESH)

    zs = [wrap(z + d, n_z) for d in range(n_z)]
    ys = [wrap(y + d, NY) for d in range(NY)]
    tps = [wrap(tp + d, n_tp) for d in range(n_tp)]
    far_first = [
        n_z // 2 + ((i + 1) // 2 if i % 2 else -((i + 1) // 2)) for i in range(n_z - 1)
    ]
    for d in far_first:
        greet(sp=zs[d] * NY + y)

    def plane(d):
        return z * NY + ys[d // n_tp], tps[d % n_tp]

    for d in range(1, NY * n_tp):
        to_sp, to_tp = plane(d)
        greet(sp=to_sp, tp=to_tp)
    cross_next = has_next & (y == NY - 1)
    cross_last = has_last & (y == 0)

    @pl.when(cross_next)
    def _():
        greet(sp=lax.rem(sp + 1, n_sp))

    @pl.when(cross_last)
    def _():
        greet(sp=lax.rem(sp + n_sp - 1, n_sp))

    own_lat = lat.at[tp]
    loads = {}
    for i, (name, src, dst) in enumerate(
        [
            ("cond", cond_hbm, cond),
            ("ctx_cond", ctx_cond_hbm, ctx_cond),
            ("shift", shift_hbm, shift_w),
            ("scale", scale_hbm, scale_w),
            ("gate", gate_hbm, gate_w),
            ("lat", latent_hbm, own_lat),
            ("row", rot_row_hbm.at[sp], rot_row),
            ("col", rot_col_hbm, rot_col),
            ("gain", gain_hbm, gain),
            ("context", context_hbm, context),
            ("wk", wk_hbm, wkv.at[:, 0:HEAD_DIM]),
            ("wv", wv_hbm, wkv.at[:, HEAD_DIM : 2 * HEAD_DIM]),
            ("wq", wq_hbm, wq),
            ("wo", wo_hbm, wo),
            ("sink", sink_hbm, sink),
        ]
    ):
        loads[name] = pltpu.make_async_copy(src, dst, load_sem.at[i])
        loads[name].start()

    def rcopy(src, dst, ssem, rsem, **where):
        return pltpu.make_async_remote_copy(
            src_ref=src,
            dst_ref=dst,
            send_sem=ssem,
            recv_sem=rsem,
            device_id=where,
            device_id_type=MESH,
        )

    def silu(v):
        return v / (1.0 + jnp.exp(-v))

    loads["cond"].wait()
    loads["ctx_cond"].wait()
    depth = cond.shape[1]
    row_id = lax.broadcasted_iota(jnp.int32, (16, depth), 0)
    active = jnp.where(
        row_id == 0,
        jnp.broadcast_to(silu(cond[...]), (16, depth)),
        jnp.broadcast_to(silu(ctx_cond[...]), (16, depth)),
    ).astype(BF16)
    vector = 0
    for name, weight, count in (("shift", shift_w, 2), ("scale", scale_w, 2), ("gate", gate_w, 1)):
        loads[name].wait()
        product = jnp.dot(active, weight[...], preferred_element_type=F32)
        for v in range(count):
            for j in range(chunks):
                z_in[z, vector * chunks + j] = product[v : v + 1, j * LANES : (j + 1) * LANES]
            vector += 1

    loads["lat"].wait()

    pl.semaphore_wait(
        barrier,
        (n_z - 1)
        + (NY * n_tp - 1)
        + cross_next.astype(jnp.int32)
        + cross_last.astype(jnp.int32),
    )

    def z_copy(d, slot):
        return rcopy(
            z_in.at[z], z_in.at[slot], z_send.at[0], z_recv.at[0], sp=zs[d] * NY + y
        )

    for d in far_first:
        z_copy(d, z).start()

    low, high = pl.ds(0, half), pl.ds(half, half)

    def lat_copy(slot, part, sem, to):
        piece = lat.at[slot, part]
        which = 0 if part is not high else 1
        return rcopy(piece, piece, lat_send.at[0], lat_recv.at[slot, which], tp=to)

    whole = pl.ds(0, rows)
    xp, xm = at_x(1, core), at_x(3, core)
    far = at_x(2, core)
    for copy in (
        lat_copy(tp, low, 0, xp),
        lat_copy(tp, high, 1, xm),
        lat_copy(tp, low, 4, partner),
        lat_copy(tp, high, 5, partner),
    ):
        copy.start()

    def lat_arrival(slot, which):
        lat_copy(slot, low if which == 0 else high, 0, partner).wait_recv()

    def invert(slot):
        floats = lat[slot].astype(F32)
        mean = jnp.mean(floats * floats, axis=-1, keepdims=True)
        inv[slot] = jnp.broadcast_to(lax.rsqrt(mean + NORM_EPS), (rows, LANES))

    wo_part = wo.shape[0] // NY // 2

    def far_weights(source, to_sp, to_tp, piece, sem):
        at = pl.ds(pl.multiple_of((2 * y + piece) * wo_part, wo_part), wo_part)
        return rcopy(
            source.at[at], wo_far.at[at], wf_send.at[0], wf_recv.at[sem], sp=to_sp, tp=to_tp
        )

    def share_far_weights(piece):
        far_weights(wo, sp, far, piece, piece).wait_recv()
        for d in (2, 1, 3):
            far_weights(wo_far, z * NY + ys[d], tp, piece, 2 + piece).start()

    loads["wo"].wait()
    far_weights(wo, sp, far, 0, 0).start()

    def rotary_and_mask():
        loads["row"].wait()
        loads["col"].wait()
        for g in range(group_rows // GRID_W):
            cos[g * GRID_W : (g + 1) * GRID_W, :] = rot_row[g : g + 1, :] + rot_col[0:GRID_W, :]
            sin[g * GRID_W : (g + 1) * GRID_W, :] = (
                rot_row[16 + g : 17 + g, :] + rot_col[GRID_W : 2 * GRID_W, :]
            )
        def mask_rows(i):
            at = pl.ds(pl.multiple_of(i * 64, 64), 64)
            shape = (64, 4 * rows)
            lane_at = lax.rem(lax.broadcasted_iota(jnp.int32, shape, 1), 2 * rows)
            row = lane_at + jnp.where(lane_at < rows, other * rows, (core - 1) * rows)
            key = lax.broadcasted_iota(jnp.int32, shape, 0) + i * 64
            bias[at, :] = jnp.where(jnp.abs(key - row - REACH) <= REACH, 0.0, MASKED_SCORE)

        loop(0, (2 * rows + 2 * REACH) // 64, mask_rows)

    rotary_and_mask()
    invert(tp)
    lat_arrival(partner, 0)
    lat_arrival(partner, 1)
    invert(partner)
    z_all = z_in.at[pl.ds(0, n_z - 1)]
    z_total = rcopy(z_all, z_all, z_send.at[0], z_recv.at[0], sp=sp)
    z_total.wait_recv()
    own_full = y * n_tp + tp
    full[own_full] = jnp.sum(z_in[...], axis=0)

    def xy_copy(d, mine):
        to_sp, to_tp = plane(d)
        peer = ys[d // n_tp] * n_tp + to_tp
        slot = own_full if mine else peer
        return rcopy(
            full.at[own_full],
            full.at[slot],
            xy_send.at[0],
            xy_recv.at[0],
            sp=to_sp,
            tp=to_tp,
        )

    for d in range(1, NY * n_tp):
        xy_copy(d, True).start()

    for part, i, to in ((high, 2, xp), (low, 3, xm)):
        copy = lat_copy(tp, part, i, to)
        copy.start()

    far_weights(wo, sp, far, 1, 1).start()

    for i, slot, order in ((0, xm, (0,)), (1, xp, (1,))):
        for j in order:
            part = (low, high)[j]
            lat_arrival(slot, j)
            copy = lat_copy(slot, part, 8 + 2 * i + j, partner)
            copy.start()
    share_far_weights(0)
    xy_all = full.at[pl.ds(0, NY * n_tp - 1)]
    xy_total = rcopy(xy_all, xy_all, xy_send.at[0], xy_recv.at[0], sp=sp)
    xy_total.wait_recv()
    for t in range(n_tp):
        sums = full[t]
        for r in range(1, NY):
            sums = sums + full[r * n_tp + t]
        for v in range(5):
            for j in range(chunks):
                column = t * columns + j * LANES
                mod[v : v + 1, column : column + LANES] = sums[v * chunks + j]
    loads["gain"].wait()
    gains = gain[...]
    mod[2:3, :] = gains * (1.0 + mod[2:3, :])
    mod[3:4, :] = gains * (1.0 + mod[3:4, :])

    def normed(block, shift_row, scale_row):
        floats = block.astype(F32)
        inverse = lax.rsqrt(jnp.mean(floats * floats, axis=-1, keepdims=True) + NORM_EPS)
        return (
            floats * inverse * mod[scale_row : scale_row + 1, :] + mod[shift_row : shift_row + 1, :]
        ).astype(BF16)

    loads["context"].wait()
    loads["wk"].wait()
    loads["wv"].wait()
    ctx_hidden[...] = normed(context[...], 1, 3)
    ctx_kv[sp] = jnp.dot(ctx_hidden[...], wkv[...], preferred_element_type=F32).astype(BF16)

    def ctx_copy(slot, peer, sem):
        return rcopy(
            ctx_kv.at[slot], ctx_kv.at[slot], ctx_send.at[0], ctx_recv.at[sem], sp=peer
        )

    def near_first(i):
        return i // 2 + 1 if i % 2 == 0 else n_z - i // 2 - 1

    def ctx_z(i):
        return ctx_copy(sp, zs[near_first(i)] * NY + y, z)

    for i in (14, 13, 12, 0, 1, 11, 10, 2, 3, 9, 8, 4, 5, 7, 6):
        ctx_z(i).start()

    relay_a = lat_copy(xm, low, 6, xp)
    relay_a.start()
    relay_b = lat_copy(xp, high, 7, xm)
    relay_b.start()

    def ctx_y(i, d):
        slot = (zs[near_first(i - 1)] if i else z) * NY + y
        return slot, ctx_copy(slot, z * NY + ys[d], n_z)

    def relay_ctx(first, last):
        for i in range(first, last):
            if i:
                of = zs[near_first(i - 1)]
                ctx_copy(of * NY + y, sp, of).wait_recv()
            for d in (2, 1, 3):
                ctx_y(i, d)[1].start()

    relay_ctx(0, 1)

    lane = lax.broadcasted_iota(jnp.int32, (2 * rows, HEAD_DIM), 1)
    quarter = HEAD_DIM // 4
    low_half = lax.rem(lane, 2 * quarter) < quarter
    strip = 32

    def turned(u, cosine, sine):
        swapped = jnp.where(
            low_half, pltpu.roll(u, HEAD_DIM - quarter, 1), pltpu.roll(u, quarter, 1)
        )
        return (u * cosine + swapped * sine).astype(BF16)

    def halo_copy(up):
        source = group_rows if up else REACH
        target = 0 if up else group_rows + REACH
        which = 0 if up else 1
        return rcopy(
            kv.at[pl.ds(source, REACH)],
            kv.at[pl.ds(target, REACH)],
            halo_send.at[which],
            halo_recv.at[which],
            sp=lax.rem(sp + (1 if up else n_sp - 1), n_sp),
        )

    def process(chip, relay_one, relay_two):

        def norm_strip(i):
            at = pl.ds(pl.multiple_of(i * strip, strip), strip)
            for c in range(2):
                inverse = inv[2 * chip + c, at, :]
                to = pl.ds(pl.multiple_of(c * rows + i * strip, strip), strip)
                for j in range(width // LANES):
                    cols = slice(j * LANES, (j + 1) * LANES)
                    hidden[to, cols] = (
                        lat[2 * chip + c, at, cols].astype(F32) * inverse * mod[2:3, cols]
                        + mod[0:1, cols]
                    ).astype(BF16)

        loop(0, rows // strip, norm_strip)
        relay_ctx(*relay_one)
        begin = pl.multiple_of(chip * 2 * rows, strip)
        here = pl.ds(begin, 2 * rows)
        kept = pl.ds(pl.multiple_of(begin + REACH, strip), 2 * rows)
        cosine, sine = cos[here, :], sin[here, :]
        pair = jnp.dot(hidden[...], wkv[...], preferred_element_type=F32)
        kv[kept, 0:HEAD_DIM] = turned(pair[:, 0:HEAD_DIM], cosine, sine)
        kv[kept, HEAD_DIM:] = pair[:, HEAD_DIM:].astype(BF16)
        q = jnp.dot(hidden[...], wq[...], preferred_element_type=F32)
        for h in range(2):
            cols = slice(h * HEAD_DIM, (h + 1) * HEAD_DIM)
            queries[here, cols] = turned(q[:, cols], cosine, sine)

        @pl.when(has_next & (chip == NX - 1))
        def _():
            halo_copy(True).start()

        @pl.when(has_last & (chip == 0))
        def _():
            halo_copy(False).start()

        relay_ctx(*relay_two)

    loads["wq"].wait()

    near = jnp.where(x < 2, NX - 1, 1)

    polls = [((0, 0), (0, 0)), ((1, 3), (3, 5)), ((5, 7), (7, 9)), ((0, 0), (0, 0))]
    for k in range(NX):
        step = (0, near, NX - near, 2)[k]
        chip = lax.rem(x + step, NX)
        slot = 2 * chip + other
        if k == 1:
            for i, neighbour, j in ((0, xm, 1), (1, xp, 0)):
                part = (low, high)[j]
                lat_arrival(neighbour, j)
                copy = lat_copy(neighbour, part, 8 + 2 * i + j, partner)
                copy.start()
            invert(xm)
            invert(xp)
        if k == 3:
            lat_arrival(far, 0)
            lat_copy(far, low, 12, partner).start()
            lat_arrival(far, 1)
            lat_copy(far, high, 13, partner).start()
            invert(far)
            relay_ctx(9, n_z)
        if k:
            lat_arrival(slot, 0)
            lat_arrival(slot, 1)
            invert(slot)
        process(chip, *polls[k])


    @pl.when(jnp.logical_not(has_last))
    def _():
        kv[0:REACH, :] = jnp.zeros((REACH, 2 * HEAD_DIM), BF16)

    @pl.when(jnp.logical_not(has_next))
    def _():
        kv[group_rows + REACH :, :] = jnp.zeros((REACH, 2 * HEAD_DIM), BF16)

    loads["sink"].wait()

    @pl.when(has_last)
    def _():
        halo_copy(True).wait_recv()

    @pl.when(has_next)
    def _():
        halo_copy(False).wait_recv()

    rest = ctx_kv.at[pl.ds(0, n_z * (NY - 1))]
    rcopy(rest, rest, ctx_send.at[0], ctx_recv.at[n_z], sp=sp).wait_recv()

    share_far_weights(1)

    span = 2 * rows + 2 * REACH
    across = (((0,), (0,)), ((), ()))
    total_rows = group_rows * n_sp
    ctx_total = n_sp * ctx_rows
    factor = HEAD_DIM ** (-0.5) * LOG2E
    contract = (((1,), (1,)), ((), ()))

    both = 2 * rows
    lanes = 2 * both

    def attend(chip):
        begin = pl.multiple_of(chip * both, strip)
        around = pl.ds(begin, span)
        given = pl.ds(pl.multiple_of(begin + other * rows, strip), rows)
        kept_at = pl.ds(pl.multiple_of(begin + core * rows, strip), rows)
        q = jnp.concatenate(
            [
                queries[at, h * HEAD_DIM : (h + 1) * HEAD_DIM]
                for h in range(2)
                for at in (given, kept_at)
            ],
            axis=0,
        )
        key_pos = (
            sp * group_rows + begin - REACH + lax.broadcasted_iota(jnp.int32, (span, LANES), 0)
        )
        edge[...] = jnp.where((key_pos < 0) | (key_pos >= total_rows), MASKED_SCORE, 0.0)
        ctx_keys = ctx_kv[:, :, 0:HEAD_DIM].reshape(ctx_total, HEAD_DIM)
        ctx_values = ctx_kv[:, :, HEAD_DIM:].reshape(ctx_total, HEAD_DIM)
        band_keys, band_values = kv[around, 0:HEAD_DIM], kv[around, HEAD_DIM:]
        sinks = jnp.concatenate(
            [jnp.broadcast_to(sink[0:1, i : i + 1] * LOG2E, (1, both)) for i in range(2)], axis=1
        )
        groups = [slice(0, 2 * LANES), slice(2 * LANES, lanes)]
        logits = []
        for g in groups:
            logits.append(
                (
                    lax.dot_general(band_keys, q[g], contract, preferred_element_type=F32),
                    lax.dot_general(ctx_keys, q[g], contract, preferred_element_type=F32),
                )
            )
        mixed = []
        for g, (band, far_logits) in zip(groups, logits):
            wide = (g.stop - g.start) // LANES
            band = band * factor + bias[:, g] + jnp.concatenate([edge[...]] * wide, axis=1)
            far_logits = far_logits * factor
            top = jnp.maximum(
                jnp.maximum(
                    jnp.max(band, axis=0, keepdims=True),
                    jnp.max(far_logits, axis=0, keepdims=True),
                ),
                sinks[:, g],
            )
            band_exp = jnp.exp2(band - top)
            far_exp = jnp.exp2(far_logits - top)
            total = (
                jnp.sum(band_exp, axis=0, keepdims=True)
                + jnp.sum(far_exp, axis=0, keepdims=True)
                + jnp.exp2(sinks[:, g] - top)
            )
            summed = lax.dot_general(
                band_values, band_exp.astype(BF16), across, preferred_element_type=F32
            ) + lax.dot_general(
                ctx_values, far_exp.astype(BF16), across, preferred_element_type=F32
            )
            mixed.append((summed / total).T.astype(BF16))
        mixed = jnp.concatenate(mixed, axis=0)
        for h in range(2):
            att[:, h * HEAD_DIM : (h + 1) * HEAD_DIM] = mixed[h * both : (h + 1) * both]

    def chip_of(k):
        return lax.rem(
            x + jnp.where(k == 0, 2, jnp.where(k == 1, 1, jnp.where(k == 2, 3, 0))), NX
        )

    def give_copy(k):
        return rcopy(give.at[k], pin.at[k], give_send.at[0], give_recv.at[k], tp=partner)

    def att_copy():
        return rcopy(att_out, att_in, att_send.at[0], att_recv.at[0], tp=far)

    n_tile = 512

    def project(k, with_far):
        for j in range(width // n_tile):
            cols = slice(j * n_tile, (j + 1) * n_tile)
            value = jnp.dot(att[...], wo[:, cols], preferred_element_type=F32)
            if with_far:
                value = value + jnp.dot(
                    att_in[...], wo_far[:, cols], preferred_element_type=F32
                )
            give[k, :, cols] = value[0:rows].astype(BF16)
            kept[:, cols] = value[rows:]
        give_copy(k).start()

    def add_given(k, store):
        give_copy(k).wait_recv()

        for i in range(rows // strip):
            at = pl.ds(i * strip, strip)
            store(at, kept[at, :] + pin[k, at, :].astype(F32))

    def chip_block(k):
        attend(chip_of(k))

        @pl.when(k == 0)
        def _():
            att_out[...] = att[...]
            att_copy().start()

        for side in range(2):

            @pl.when(k == 2 + side)
            def _():
                def store(at, value):
                    outx[side, at, :] = value.astype(BF16)
                    rcopy(
                        outx.at[side, at],
                        x_in.at[side, at],
                        xs_send.at[0],
                        xs_recv.at[0],
                        tp=xm if side else xp,
                    ).start()

                add_given(side, store)

        @pl.when((k == 1) | (k == 2))
        def _():
            project(k - 1, False)


    loop(0, NX, chip_block)

    att_copy().wait_recv()
    shared = wo_far.at[pl.ds(0, (NY - 1) * wo_part)]
    for sem in (2, 3):
        rcopy(shared, shared, wf_send.at[0], wf_recv.at[sem], sp=sp).wait_recv()
    project(2, True)

    z_total.wait_send()
    xy_total.wait_send()
    sent = lat.at[pl.ds(0, 7)]
    rcopy(sent, sent, lat_send.at[0], lat_recv.at[0, 0], sp=sp).wait_send()
    sent = ctx_kv.at[pl.ds(0, n_z * NY - 1)]
    rcopy(sent, sent, ctx_send.at[0], ctx_recv.at[0], sp=sp).wait_send()

    @pl.when(has_next)
    def _():
        halo_copy(True).wait_send()

    @pl.when(has_last)
    def _():
        halo_copy(False).wait_send()

    def whole_copy(ref, ssem, rsem):
        return rcopy(ref, ref, ssem, rsem, sp=sp)

    def own_store(at, value):
        kept[at, :] = value

    add_given(2, own_store)
    whole_copy(x_in, xs_send.at[0], xs_recv.at[0]).wait_recv()

    def finish(i):
        at = pl.ds(pl.multiple_of(i * strip, strip), strip)
        mixed = kept[at, :] + x_in[0, at, :].astype(F32) + x_in[1, at, :].astype(F32)
        out_ref[at, :] = (lat[tp, at, :].astype(F32) + mod[4:5, :] * mixed).astype(BF16)

    loop(0, rows // strip, finish)

    whole_copy(give, give_send.at[0], give_recv.at[0]).wait_send()
    whole_copy(outx, xs_send.at[0], xs_recv.at[0]).wait_send()
    whole_copy(wo_far, wf_send.at[0], wf_recv.at[0]).wait_send()
    att_copy().wait_send()


def angle_tables(total_rows, n_sp):
    inv_freq = np.power(
        10000.0, -np.arange(0, HEAD_DIM // 2, 2, dtype=np.float64) / (HEAD_DIM // 2)
    ).astype(np.float32)

    def tables(count):
        angle = (np.arange(count, dtype=np.float32)[:, None] * inv_freq).astype(np.float64)
        cosine, sine = np.cos(angle), np.sin(angle)
        return (
            np.concatenate([cosine, cosine], axis=1).astype(np.float32),
            np.concatenate([-sine, sine], axis=1).astype(np.float32),
        )

    half = HEAD_DIM // 2
    grid_rows = total_rows // GRID_W
    per = grid_rows // n_sp
    by_row, by_col = tables(grid_rows), tables(GRID_W)
    rows = np.zeros((n_sp, 32, HEAD_DIM), np.float32)
    rows[:, 0:per, :half] = by_row[0].reshape(n_sp, per, half)
    rows[:, 16 : 16 + per, :half] = by_row[1].reshape(n_sp, per, half)
    cols = np.zeros((2 * GRID_W, HEAD_DIM), np.float32)
    cols[:GRID_W, half:] = by_col[0]
    cols[GRID_W:, half:] = by_col[1]
    return rows, cols


def shards(
    n_sp,
    n_tp,
    latent,
    condition,
    context_condition,
    context,
    norm_gain,
    shift_weight,
    scale_weight,
    gate_weight,
    query_weight,
    key_matrix,
    value_matrix,
    sink_logit_head,
    out_weight,
):
    rows, width = latent.shape
    group_rows = rows * n_tp
    rot_rows, rot_cols = angle_tables(group_rows * n_sp, n_sp)
    columns = shift_weight.shape[1]
    groups = 5 * columns // LANES
    query_width = query_weight.shape[1]
    ctx_rows = context.shape[0]
    n_z = n_sp // NY
    dma = pltpu.SemaphoreType.DMA
    vmem = pl.BlockSpec(memory_space=pltpu.VMEM)
    anywhere = pl.BlockSpec(memory_space=pltpu.HBM)
    def like(array):
        return pltpu.VMEM(array.shape, array.dtype)

    condition = condition.reshape(1, -1)
    context_condition = context_condition.reshape(1, -1)
    norm_gain = norm_gain.reshape(1, -1)
    sink = sink_logit_head.reshape(1, -1)
    return pl.pallas_call(
        functools.partial(block_kernel, n_sp, n_tp),
        out_shape=pltpu.VMEM((rows, width), BF16),
        in_specs=[anywhere] * 15,
        out_specs=vmem,
        scratch_shapes=[
            like(condition),
            like(context_condition),
            like(norm_gain),
            like(sink),
            pltpu.VMEM((32, HEAD_DIM), F32),
            pltpu.VMEM((2 * GRID_W, HEAD_DIM), F32),
            pltpu.VMEM((group_rows, HEAD_DIM), F32),
            pltpu.VMEM((group_rows, HEAD_DIM), F32),
            like(context),
            like(shift_weight),
            like(scale_weight),
            like(gate_weight),
            like(query_weight),
            pltpu.VMEM((width, 2 * HEAD_DIM), BF16),
            like(out_weight),
            pltpu.VMEM((n_tp, rows, width), BF16),
            pltpu.VMEM((n_z, groups, 1, LANES), F32),
            pltpu.VMEM((NY * n_tp, groups, 1, LANES), F32),
            pltpu.VMEM((n_tp, rows, LANES), F32),
            pltpu.VMEM((8, width), F32),
            pltpu.VMEM((2 * rows, width), BF16),
            like(context),
            pltpu.VMEM((group_rows, query_width), BF16),
            pltpu.VMEM((group_rows + 2 * REACH, 2 * HEAD_DIM), BF16),
            pltpu.VMEM((n_sp, ctx_rows, 2 * HEAD_DIM), BF16),
            pltpu.VMEM((2 * rows, query_width), BF16),
            pltpu.VMEM((3, rows, width), BF16),
            pltpu.VMEM((3, rows, width), BF16),
            pltpu.VMEM((2, rows, width), BF16),
            pltpu.VMEM((2, rows, width), BF16),
            pltpu.VMEM((2 * rows, query_width), BF16),
            pltpu.VMEM((2 * rows, query_width), BF16),
            like(out_weight),
            pltpu.VMEM((rows, width), F32),
            pltpu.VMEM((2 * rows + 2 * REACH, 4 * rows), F32),
            pltpu.VMEM((2 * rows + 2 * REACH, LANES), F32),
            dma((15,)),
            dma((1,)),
            dma((1,)),
            dma((1,)),
            dma((1,)),
            dma((1,)),
            dma((n_tp, 2)),
            dma((1,)),
            dma((n_z + 1,)),
            dma((2,)),
            dma((2,)),
            dma((1,)),
            dma((3,)),
            dma((1,)),
            dma((1,)),
            dma((1,)),
            dma((1,)),
            dma((1,)),
            dma((4,)),
        ],
        compiler_params=pltpu.CompilerParams(
            collective_id=0, has_side_effects=True, vmem_limit_bytes=int(60 * 1024 * 1024)
        ),
    )(
        condition,
        context_condition,
        norm_gain,
        sink,
        jnp.asarray(rot_rows),
        jnp.asarray(rot_cols),
        latent,
        context,
        shift_weight,
        scale_weight,
        gate_weight,
        query_weight,
        key_matrix,
        value_matrix,
        out_weight,
    )


def solution(mesh):
    placed = (
        P(("sp", "tp"), None),
        P("sp"),
        P("sp"),
        P("sp", None),
        P(),
        P("sp", "tp"),
        P("sp", "tp"),
        P("sp", "tp"),
        P(None, "tp"),
        P(None, "tp"),
        P(None, "tp"),
        P("tp"),
        P("tp", None),
    )
    return jax.shard_map(
        functools.partial(shards, mesh.shape["sp"], mesh.shape["tp"]),
        mesh=mesh,
        in_specs=placed,
        out_specs=P(("sp", "tp"), None),
        check_vma=False,
    )
```

```python
import functools

import jax
import jax.numpy as jnp
import numpy as np
from jax import lax
from jax.experimental import pallas as pl
from jax.experimental.pallas import tpu as pltpu
from jax.sharding import PartitionSpec as P

HEAD_DIM = 128
REACH = 128
GRID_W = 64
NORM_EPS = 1e-05
MASKED_SCORE = -1e30
LANES = 128
NY = 4
NX = 4
MESH = pl.DeviceIdType.MESH
F32 = jnp.float32
BF16 = jnp.bfloat16
LOG2E = 1.4426950408889634


def loop(low, high, f):
    def step(i, carry):
        f(i)
        return carry

    lax.fori_loop(low, high, step, 0)


def block_kernel(
    n_sp,
    n_tp,
    cond_hbm,
    ctx_cond_hbm,
    gain_hbm,
    sink_hbm,
    rot_row_hbm,
    rot_col_hbm,
    latent_hbm,
    context_hbm,
    shift_hbm,
    scale_hbm,
    gate_hbm,
    wq_hbm,
    wk_hbm,
    wv_hbm,
    wo_hbm,
    out_ref,
    cond,
    ctx_cond,
    gain,
    sink,
    rot_row,
    rot_col,
    cos,
    sin,
    context,
    shift_w,
    scale_w,
    gate_w,
    wq,
    wkv,
    wo,
    lat,
    z_in,
    full,
    inv,
    mod,
    hidden,
    ctx_hidden,
    queries,
    kv,
    ctx_kv,
    att,
    give,
    pin,
    outx,
    x_in,
    att_out,
    att_in,
    wo_far,
    kept,
    bias,
    edge,
    load_sem,
    z_send,
    z_recv,
    xy_send,
    xy_recv,
    lat_send,
    lat_recv,
    ctx_send,
    ctx_recv,
    halo_send,
    halo_recv,
    give_send,
    give_recv,
    xs_send,
    xs_recv,
    att_send,
    att_recv,
    wf_send,
    wf_recv,
):
    sp = lax.axis_index("sp")
    tp = lax.axis_index("tp")
    n_z = n_sp // NY
    z, x = sp // NY, tp // 2
    y, core = sp - NY * z, tp - 2 * x
    other = 1 - core
    partner = 2 * x + other

    def wrap(i, n):
        return jnp.where(i >= n, i - n, i)

    def at_x(dx, c):
        return 2 * wrap(x + dx, NX) + c

    slots, rows, width = lat.shape
    group_rows = rows * n_tp
    half = rows // 2
    columns = shift_w.shape[1]
    chunks = columns // LANES
    ctx_rows = context.shape[0]
    has_next, has_last = sp < n_sp - 1, sp > 0

    barrier = pltpu.get_barrier_semaphore()

    def greet(**where):
        pl.semaphore_signal(barrier, inc=1, device_id=where, device_id_type=MESH)

    zs = [wrap(z + d, n_z) for d in range(n_z)]
    ys = [wrap(y + d, NY) for d in range(NY)]
    tps = [wrap(tp + d, n_tp) for d in range(n_tp)]
    far_first = [
        n_z // 2 + ((i + 1) // 2 if i % 2 else -((i + 1) // 2)) for i in range(n_z - 1)
    ]
    for d in far_first:
        greet(sp=zs[d] * NY + y)

    def plane(d):
        return z * NY + ys[d // n_tp], tps[d % n_tp]

    for d in range(1, NY * n_tp):
        to_sp, to_tp = plane(d)
        greet(sp=to_sp, tp=to_tp)
    cross_next = has_next & (y == NY - 1)
    cross_last = has_last & (y == 0)

    @pl.when(cross_next)
    def _():
        greet(sp=lax.rem(sp + 1, n_sp))

    @pl.when(cross_last)
    def _():
        greet(sp=lax.rem(sp + n_sp - 1, n_sp))

    own_lat = lat.at[tp]
    loads = {}
    for i, (name, src, dst) in enumerate(
        [
            ("cond", cond_hbm, cond),
            ("ctx_cond", ctx_cond_hbm, ctx_cond),
            ("shift", shift_hbm, shift_w),
            ("scale", scale_hbm, scale_w),
            ("gate", gate_hbm, gate_w),
            ("lat", latent_hbm, own_lat),
            ("row", rot_row_hbm.at[sp], rot_row),
            ("col", rot_col_hbm, rot_col),
            ("gain", gain_hbm, gain),
            ("context", context_hbm, context),
            ("wk", wk_hbm, wkv.at[:, 0:HEAD_DIM]),
            ("wv", wv_hbm, wkv.at[:, HEAD_DIM : 2 * HEAD_DIM]),
            ("wq", wq_hbm, wq),
            ("wo", wo_hbm, wo),
            ("sink", sink_hbm, sink),
        ]
    ):
        loads[name] = pltpu.make_async_copy(src, dst, load_sem.at[i])
        loads[name].start()

    def rcopy(src, dst, ssem, rsem, **where):
        return pltpu.make_async_remote_copy(
            src_ref=src,
            dst_ref=dst,
            send_sem=ssem,
            recv_sem=rsem,
            device_id=where,
            device_id_type=MESH,
        )

    def silu(v):
        return v / (1.0 + jnp.exp(-v))

    loads["cond"].wait()
    loads["ctx_cond"].wait()
    depth = cond.shape[1]
    row_id = lax.broadcasted_iota(jnp.int32, (16, depth), 0)
    active = jnp.where(
        row_id == 0,
        jnp.broadcast_to(silu(cond[...]), (16, depth)),
        jnp.broadcast_to(silu(ctx_cond[...]), (16, depth)),
    ).astype(BF16)
    vector = 0
    for name, weight, count in (("shift", shift_w, 2), ("scale", scale_w, 2), ("gate", gate_w, 1)):
        loads[name].wait()
        product = jnp.dot(active, weight[...], preferred_element_type=F32)
        for v in range(count):
            for j in range(chunks):
                z_in[z, vector * chunks + j] = product[v : v + 1, j * LANES : (j + 1) * LANES]
            vector += 1

    loads["lat"].wait()

    pl.semaphore_wait(
        barrier,
        (n_z - 1)
        + (NY * n_tp - 1)
        + cross_next.astype(jnp.int32)
        + cross_last.astype(jnp.int32),
    )

    def z_copy(d, slot):
        return rcopy(
            z_in.at[z], z_in.at[slot], z_send.at[0], z_recv.at[0], sp=zs[d] * NY + y
        )

    for d in far_first:
        z_copy(d, z).start()

    low, high = pl.ds(0, half), pl.ds(half, half)

    def lat_copy(slot, part, sem, to):
        piece = lat.at[slot, part]
        which = 0 if part is not high else 1
        return rcopy(piece, piece, lat_send.at[0], lat_recv.at[slot, which], tp=to)

    whole = pl.ds(0, rows)
    xp, xm = at_x(1, core), at_x(3, core)
    far = at_x(2, core)
    for copy in (
        lat_copy(tp, low, 0, xp),
        lat_copy(tp, high, 1, xm),
        lat_copy(tp, low, 4, partner),
        lat_copy(tp, high, 5, partner),
    ):
        copy.start()

    def lat_arrival(slot, which):
        lat_copy(slot, low if which == 0 else high, 0, partner).wait_recv()

    def invert(slot):
        floats = lat[slot].astype(F32)
        mean = jnp.mean(floats * floats, axis=-1, keepdims=True)
        inv[slot] = jnp.broadcast_to(lax.rsqrt(mean + NORM_EPS), (rows, LANES))

    wo_part = wo.shape[0] // NY // 2

    def far_weights(source, to_sp, to_tp, piece, sem):
        at = pl.ds(pl.multiple_of((2 * y + piece) * wo_part, wo_part), wo_part)
        return rcopy(
            source.at[at], wo_far.at[at], wf_send.at[0], wf_recv.at[sem], sp=to_sp, tp=to_tp
        )

    def share_far_weights(piece):
        far_weights(wo, sp, far, piece, piece).wait_recv()
        for d in (2, 1, 3):
            far_weights(wo_far, z * NY + ys[d], tp, piece, 2 + piece).start()

    loads["wo"].wait()
    far_weights(wo, sp, far, 0, 0).start()

    def rotary_and_mask():
        loads["row"].wait()
        loads["col"].wait()
        for g in range(group_rows // GRID_W):
            cos[g * GRID_W : (g + 1) * GRID_W, :] = rot_row[g : g + 1, :] + rot_col[0:GRID_W, :]
            sin[g * GRID_W : (g + 1) * GRID_W, :] = (
                rot_row[16 + g : 17 + g, :] + rot_col[GRID_W : 2 * GRID_W, :]
            )
        def mask_rows(i):
            at = pl.ds(pl.multiple_of(i * 64, 64), 64)
            shape = (64, 4 * rows)
            lane_at = lax.rem(lax.broadcasted_iota(jnp.int32, shape, 1), 2 * rows)
            row = lane_at + jnp.where(lane_at < rows, other * rows, (core - 1) * rows)
            key = lax.broadcasted_iota(jnp.int32, shape, 0) + i * 64
            bias[at, :] = jnp.where(jnp.abs(key - row - REACH) <= REACH, 0.0, MASKED_SCORE)

        loop(0, (2 * rows + 2 * REACH) // 64, mask_rows)

    rotary_and_mask()
    invert(tp)
    lat_arrival(partner, 0)
    lat_arrival(partner, 1)
    invert(partner)
    z_all = z_in.at[pl.ds(0, n_z - 1)]
    z_total = rcopy(z_all, z_all, z_send.at[0], z_recv.at[0], sp=sp)
    z_total.wait_recv()
    own_full = y * n_tp + tp
    full[own_full] = jnp.sum(z_in[...], axis=0)

    def xy_copy(d, mine):
        to_sp, to_tp = plane(d)
        peer = ys[d // n_tp] * n_tp + to_tp
        slot = own_full if mine else peer
        return rcopy(
            full.at[own_full],
            full.at[slot],
            xy_send.at[0],
            xy_recv.at[0],
            sp=to_sp,
            tp=to_tp,
        )

    for dy in (2, 1, 3, 0):
        for dt in (4, 3, 5, 2, 6, 1, 7, 0):
            if dy or dt:
                xy_copy(dy * n_tp + dt, True).start()

    for part, i, to in ((high, 2, xp), (low, 3, xm)):
        copy = lat_copy(tp, part, i, to)
        copy.start()

    for i, slot, order in ((0, xm, (0,)), (1, xp, (1,))):
        for j in order:
            part = (low, high)[j]
            lat_arrival(slot, j)
            copy = lat_copy(slot, part, 8 + 2 * i + j, partner)
            copy.start()
    share_far_weights(0)
    xy_all = full.at[pl.ds(0, NY * n_tp - 1)]
    xy_total = rcopy(xy_all, xy_all, xy_send.at[0], xy_recv.at[0], sp=sp)
    xy_total.wait_recv()
    for t in range(n_tp):
        sums = full[t]
        for r in range(1, NY):
            sums = sums + full[r * n_tp + t]
        for v in range(5):
            for j in range(chunks):
                column = t * columns + j * LANES
                mod[v : v + 1, column : column + LANES] = sums[v * chunks + j]
    loads["gain"].wait()
    gains = gain[...]
    mod[2:3, :] = gains * (1.0 + mod[2:3, :])
    mod[3:4, :] = gains * (1.0 + mod[3:4, :])

    def normed(block, shift_row, scale_row):
        floats = block.astype(F32)
        inverse = lax.rsqrt(jnp.mean(floats * floats, axis=-1, keepdims=True) + NORM_EPS)
        return (
            floats * inverse * mod[scale_row : scale_row + 1, :] + mod[shift_row : shift_row + 1, :]
        ).astype(BF16)

    loads["context"].wait()
    loads["wk"].wait()
    loads["wv"].wait()
    ctx_hidden[...] = normed(context[...], 1, 3)
    ctx_kv[sp] = jnp.dot(ctx_hidden[...], wkv[...], preferred_element_type=F32).astype(BF16)

    def ctx_copy(slot, peer, sem):
        return rcopy(
            ctx_kv.at[slot], ctx_kv.at[slot], ctx_send.at[0], ctx_recv.at[sem], sp=peer
        )

    def near_first(i):
        return i // 2 + 1 if i % 2 == 0 else n_z - i // 2 - 1

    def ctx_z(i):
        return ctx_copy(sp, zs[near_first(i)] * NY + y, z)

    for i in (14, 13, 12, 0, 1, 11, 10, 2, 3, 9, 8, 4, 5, 7, 6):
        ctx_z(i).start()

    relay_a = lat_copy(xm, low, 6, xp)
    relay_a.start()
    relay_b = lat_copy(xp, high, 7, xm)
    relay_b.start()
    far_weights(wo, sp, far, 1, 1).start()

    def ctx_y(i, d):
        slot = (zs[near_first(i - 1)] if i else z) * NY + y
        return slot, ctx_copy(slot, z * NY + ys[d], n_z)

    def relay_ctx(first, last):
        for i in range(first, last):
            if i:
                of = zs[near_first(i - 1)]
                ctx_copy(of * NY + y, sp, of).wait_recv()
            for d in (2, 1, 3):
                ctx_y(i, d)[1].start()

    relay_ctx(0, 1)

    lane = lax.broadcasted_iota(jnp.int32, (2 * rows, HEAD_DIM), 1)
    quarter = HEAD_DIM // 4
    low_half = lax.rem(lane, 2 * quarter) < quarter
    strip = 32

    def turned(u, cosine, sine):
        swapped = jnp.where(
            low_half, pltpu.roll(u, HEAD_DIM - quarter, 1), pltpu.roll(u, quarter, 1)
        )
        return (u * cosine + swapped * sine).astype(BF16)

    def halo_copy(up):
        source = group_rows if up else REACH
        target = 0 if up else group_rows + REACH
        which = 0 if up else 1
        return rcopy(
            kv.at[pl.ds(source, REACH)],
            kv.at[pl.ds(target, REACH)],
            halo_send.at[which],
            halo_recv.at[which],
            sp=lax.rem(sp + (1 if up else n_sp - 1), n_sp),
        )

    def process(chip, relay_one, relay_two):

        def norm_strip(i):
            at = pl.ds(pl.multiple_of(i * strip, strip), strip)
            for c in range(2):
                inverse = inv[2 * chip + c, at, :]
                to = pl.ds(pl.multiple_of(c * rows + i * strip, strip), strip)
                for j in range(width // LANES):
                    cols = slice(j * LANES, (j + 1) * LANES)
                    hidden[to, cols] = (
                        lat[2 * chip + c, at, cols].astype(F32) * inverse * mod[2:3, cols]
                        + mod[0:1, cols]
                    ).astype(BF16)

        loop(0, rows // strip, norm_strip)
        relay_ctx(*relay_one)
        begin = pl.multiple_of(chip * 2 * rows, strip)
        here = pl.ds(begin, 2 * rows)
        kept = pl.ds(pl.multiple_of(begin + REACH, strip), 2 * rows)
        cosine, sine = cos[here, :], sin[here, :]
        pair = jnp.dot(hidden[...], wkv[...], preferred_element_type=F32)
        kv[kept, 0:HEAD_DIM] = turned(pair[:, 0:HEAD_DIM], cosine, sine)
        kv[kept, HEAD_DIM:] = pair[:, HEAD_DIM:].astype(BF16)
        q = jnp.dot(hidden[...], wq[...], preferred_element_type=F32)
        for h in range(2):
            cols = slice(h * HEAD_DIM, (h + 1) * HEAD_DIM)
            queries[here, cols] = turned(q[:, cols], cosine, sine)

        @pl.when(has_next & (chip == NX - 1))
        def _():
            halo_copy(True).start()

        @pl.when(has_last & (chip == 0))
        def _():
            halo_copy(False).start()

        relay_ctx(*relay_two)

    loads["wq"].wait()

    near = jnp.where(x < 2, NX - 1, 1)

    polls = [((0, 0), (0, 0)), ((1, 3), (3, 5)), ((5, 7), (7, 9)), ((0, 0), (0, 0))]
    for k in range(NX):
        step = (0, near, NX - near, 2)[k]
        chip = lax.rem(x + step, NX)
        slot = 2 * chip + other
        if k == 1:
            for i, neighbour, j in ((0, xm, 1), (1, xp, 0)):
                part = (low, high)[j]
                lat_arrival(neighbour, j)
                copy = lat_copy(neighbour, part, 8 + 2 * i + j, partner)
                copy.start()
            invert(xm)
            invert(xp)
        if k == 3:
            lat_arrival(far, 0)
            lat_copy(far, low, 12, partner).start()
            lat_arrival(far, 1)
            lat_copy(far, high, 13, partner).start()
            invert(far)
            relay_ctx(9, n_z)
        if k:
            lat_arrival(slot, 0)
            lat_arrival(slot, 1)
            invert(slot)
        process(chip, *polls[k])


    @pl.when(jnp.logical_not(has_last))
    def _():
        kv[0:REACH, :] = jnp.zeros((REACH, 2 * HEAD_DIM), BF16)

    @pl.when(jnp.logical_not(has_next))
    def _():
        kv[group_rows + REACH :, :] = jnp.zeros((REACH, 2 * HEAD_DIM), BF16)

    loads["sink"].wait()

    @pl.when(has_last)
    def _():
        halo_copy(True).wait_recv()

    @pl.when(has_next)
    def _():
        halo_copy(False).wait_recv()

    rest = ctx_kv.at[pl.ds(0, n_z * (NY - 1))]
    rcopy(rest, rest, ctx_send.at[0], ctx_recv.at[n_z], sp=sp).wait_recv()

    share_far_weights(1)

    span = 2 * rows + 2 * REACH
    across = (((0,), (0,)), ((), ()))
    total_rows = group_rows * n_sp
    ctx_total = n_sp * ctx_rows
    factor = HEAD_DIM ** (-0.5) * LOG2E
    contract = (((1,), (1,)), ((), ()))

    both = 2 * rows
    lanes = 2 * both

    def attend(chip):
        begin = pl.multiple_of(chip * both, strip)
        around = pl.ds(begin, span)
        given = pl.ds(pl.multiple_of(begin + other * rows, strip), rows)
        kept_at = pl.ds(pl.multiple_of(begin + core * rows, strip), rows)
        q = jnp.concatenate(
            [
                queries[at, h * HEAD_DIM : (h + 1) * HEAD_DIM]
                for h in range(2)
                for at in (given, kept_at)
            ],
            axis=0,
        )
        key_pos = (
            sp * group_rows + begin - REACH + lax.broadcasted_iota(jnp.int32, (span, LANES), 0)
        )
        edge[...] = jnp.where((key_pos < 0) | (key_pos >= total_rows), MASKED_SCORE, 0.0)
        ctx_keys = ctx_kv[:, :, 0:HEAD_DIM].reshape(ctx_total, HEAD_DIM)
        ctx_values = ctx_kv[:, :, HEAD_DIM:].reshape(ctx_total, HEAD_DIM)
        band_keys, band_values = kv[around, 0:HEAD_DIM], kv[around, HEAD_DIM:]
        sinks = jnp.concatenate(
            [jnp.broadcast_to(sink[0:1, i : i + 1] * LOG2E, (1, both)) for i in range(2)], axis=1
        )
        groups = [slice(0, 2 * LANES), slice(2 * LANES, lanes)]
        logits = []
        for g in groups:
            logits.append(
                (
                    lax.dot_general(band_keys, q[g], contract, preferred_element_type=F32),
                    lax.dot_general(ctx_keys, q[g], contract, preferred_element_type=F32),
                )
            )
        mixed = []
        for g, (band, far_logits) in zip(groups, logits):
            wide = (g.stop - g.start) // LANES
            band = band * factor + bias[:, g] + jnp.concatenate([edge[...]] * wide, axis=1)
            far_logits = far_logits * factor
            top = jnp.maximum(
                jnp.maximum(
                    jnp.max(band, axis=0, keepdims=True),
                    jnp.max(far_logits, axis=0, keepdims=True),
                ),
                sinks[:, g],
            )
            band_exp = jnp.exp2(band - top)
            far_exp = jnp.exp2(far_logits - top)
            total = (
                jnp.sum(band_exp, axis=0, keepdims=True)
                + jnp.sum(far_exp, axis=0, keepdims=True)
                + jnp.exp2(sinks[:, g] - top)
            )
            summed = lax.dot_general(
                band_values, band_exp.astype(BF16), across, preferred_element_type=F32
            ) + lax.dot_general(
                ctx_values, far_exp.astype(BF16), across, preferred_element_type=F32
            )
            mixed.append((summed / total).T.astype(BF16))
        mixed = jnp.concatenate(mixed, axis=0)
        for h in range(2):
            att[:, h * HEAD_DIM : (h + 1) * HEAD_DIM] = mixed[h * both : (h + 1) * both]

    def chip_of(k):
        return lax.rem(
            x + jnp.where(k == 0, 2, jnp.where(k == 1, 1, jnp.where(k == 2, 3, 0))), NX
        )

    def give_copy(k):
        return rcopy(give.at[k], pin.at[k], give_send.at[0], give_recv.at[k], tp=partner)

    def att_copy():
        return rcopy(att_out, att_in, att_send.at[0], att_recv.at[0], tp=far)

    n_tile = 512

    def project(k, with_far):
        for j in range(width // n_tile):
            cols = slice(j * n_tile, (j + 1) * n_tile)
            value = jnp.dot(att[...], wo[:, cols], preferred_element_type=F32)
            if with_far:
                value = value + jnp.dot(
                    att_in[...], wo_far[:, cols], preferred_element_type=F32
                )
            give[k, :, cols] = value[0:rows].astype(BF16)
            kept[:, cols] = value[rows:]
        give_copy(k).start()

    def add_given(k, store):
        give_copy(k).wait_recv()

        for i in range(rows // strip):
            at = pl.ds(i * strip, strip)
            store(at, kept[at, :] + pin[k, at, :].astype(F32))

    def chip_block(k):
        attend(chip_of(k))

        @pl.when(k == 0)
        def _():
            att_out[...] = att[...]
            att_copy().start()

        for side in range(2):

            @pl.when(k == 2 + side)
            def _():
                def store(at, value):
                    outx[side, at, :] = value.astype(BF16)
                    rcopy(
                        outx.at[side, at],
                        x_in.at[side, at],
                        xs_send.at[0],
                        xs_recv.at[0],
                        tp=xm if side else xp,
                    ).start()

                add_given(side, store)

        @pl.when((k == 1) | (k == 2))
        def _():
            project(k - 1, False)


    loop(0, NX, chip_block)

    att_copy().wait_recv()
    shared = wo_far.at[pl.ds(0, (NY - 1) * wo_part)]
    for sem in (2, 3):
        rcopy(shared, shared, wf_send.at[0], wf_recv.at[sem], sp=sp).wait_recv()
    project(2, True)

    z_total.wait_send()
    xy_total.wait_send()
    sent = lat.at[pl.ds(0, 7)]
    rcopy(sent, sent, lat_send.at[0], lat_recv.at[0, 0], sp=sp).wait_send()
    sent = ctx_kv.at[pl.ds(0, n_z * NY - 1)]
    rcopy(sent, sent, ctx_send.at[0], ctx_recv.at[0], sp=sp).wait_send()

    @pl.when(has_next)
    def _():
        halo_copy(True).wait_send()

    @pl.when(has_last)
    def _():
        halo_copy(False).wait_send()

    def whole_copy(ref, ssem, rsem):
        return rcopy(ref, ref, ssem, rsem, sp=sp)

    def own_store(at, value):
        kept[at, :] = value

    add_given(2, own_store)
    whole_copy(x_in, xs_send.at[0], xs_recv.at[0]).wait_recv()

    def finish(i):
        at = pl.ds(pl.multiple_of(i * strip, strip), strip)
        mixed = kept[at, :] + x_in[0, at, :].astype(F32) + x_in[1, at, :].astype(F32)
        out_ref[at, :] = (lat[tp, at, :].astype(F32) + mod[4:5, :] * mixed).astype(BF16)

    loop(0, rows // strip, finish)

    whole_copy(give, give_send.at[0], give_recv.at[0]).wait_send()
    whole_copy(outx, xs_send.at[0], xs_recv.at[0]).wait_send()
    whole_copy(wo_far, wf_send.at[0], wf_recv.at[0]).wait_send()
    att_copy().wait_send()


def angle_tables(total_rows, n_sp):
    inv_freq = np.power(
        10000.0, -np.arange(0, HEAD_DIM // 2, 2, dtype=np.float64) / (HEAD_DIM // 2)
    ).astype(np.float32)

    def tables(count):
        angle = (np.arange(count, dtype=np.float32)[:, None] * inv_freq).astype(np.float64)
        cosine, sine = np.cos(angle), np.sin(angle)
        return (
            np.concatenate([cosine, cosine], axis=1).astype(np.float32),
            np.concatenate([-sine, sine], axis=1).astype(np.float32),
        )

    half = HEAD_DIM // 2
    grid_rows = total_rows // GRID_W
    per = grid_rows // n_sp
    by_row, by_col = tables(grid_rows), tables(GRID_W)
    rows = np.zeros((n_sp, 32, HEAD_DIM), np.float32)
    rows[:, 0:per, :half] = by_row[0].reshape(n_sp, per, half)
    rows[:, 16 : 16 + per, :half] = by_row[1].reshape(n_sp, per, half)
    cols = np.zeros((2 * GRID_W, HEAD_DIM), np.float32)
    cols[:GRID_W, half:] = by_col[0]
    cols[GRID_W:, half:] = by_col[1]
    return rows, cols


def shards(
    n_sp,
    n_tp,
    latent,
    condition,
    context_condition,
    context,
    norm_gain,
    shift_weight,
    scale_weight,
    gate_weight,
    query_weight,
    key_matrix,
    value_matrix,
    sink_logit_head,
    out_weight,
):
    rows, width = latent.shape
    group_rows = rows * n_tp
    rot_rows, rot_cols = angle_tables(group_rows * n_sp, n_sp)
    columns = shift_weight.shape[1]
    groups = 5 * columns // LANES
    query_width = query_weight.shape[1]
    ctx_rows = context.shape[0]
    n_z = n_sp // NY
    dma = pltpu.SemaphoreType.DMA
    vmem = pl.BlockSpec(memory_space=pltpu.VMEM)
    anywhere = pl.BlockSpec(memory_space=pltpu.HBM)
    def like(array):
        return pltpu.VMEM(array.shape, array.dtype)

    condition = condition.reshape(1, -1)
    context_condition = context_condition.reshape(1, -1)
    norm_gain = norm_gain.reshape(1, -1)
    sink = sink_logit_head.reshape(1, -1)
    return pl.pallas_call(
        functools.partial(block_kernel, n_sp, n_tp),
        out_shape=pltpu.VMEM((rows, width), BF16),
        in_specs=[anywhere] * 15,
        out_specs=vmem,
        scratch_shapes=[
            like(condition),
            like(context_condition),
            like(norm_gain),
            like(sink),
            pltpu.VMEM((32, HEAD_DIM), F32),
            pltpu.VMEM((2 * GRID_W, HEAD_DIM), F32),
            pltpu.VMEM((group_rows, HEAD_DIM), F32),
            pltpu.VMEM((group_rows, HEAD_DIM), F32),
            like(context),
            like(shift_weight),
            like(scale_weight),
            like(gate_weight),
            like(query_weight),
            pltpu.VMEM((width, 2 * HEAD_DIM), BF16),
            like(out_weight),
            pltpu.VMEM((n_tp, rows, width), BF16),
            pltpu.VMEM((n_z, groups, 1, LANES), F32),
            pltpu.VMEM((NY * n_tp, groups, 1, LANES), F32),
            pltpu.VMEM((n_tp, rows, LANES), F32),
            pltpu.VMEM((8, width), F32),
            pltpu.VMEM((2 * rows, width), BF16),
            like(context),
            pltpu.VMEM((group_rows, query_width), BF16),
            pltpu.VMEM((group_rows + 2 * REACH, 2 * HEAD_DIM), BF16),
            pltpu.VMEM((n_sp, ctx_rows, 2 * HEAD_DIM), BF16),
            pltpu.VMEM((2 * rows, query_width), BF16),
            pltpu.VMEM((3, rows, width), BF16),
            pltpu.VMEM((3, rows, width), BF16),
            pltpu.VMEM((2, rows, width), BF16),
            pltpu.VMEM((2, rows, width), BF16),
            pltpu.VMEM((2 * rows, query_width), BF16),
            pltpu.VMEM((2 * rows, query_width), BF16),
            like(out_weight),
            pltpu.VMEM((rows, width), F32),
            pltpu.VMEM((2 * rows + 2 * REACH, 4 * rows), F32),
            pltpu.VMEM((2 * rows + 2 * REACH, LANES), F32),
            dma((15,)),
            dma((1,)),
            dma((1,)),
            dma((1,)),
            dma((1,)),
            dma((1,)),
            dma((n_tp, 2)),
            dma((1,)),
            dma((n_z + 1,)),
            dma((2,)),
            dma((2,)),
            dma((1,)),
            dma((3,)),
            dma((1,)),
            dma((1,)),
            dma((1,)),
            dma((1,)),
            dma((1,)),
            dma((4,)),
        ],
        compiler_params=pltpu.CompilerParams(
            collective_id=0, has_side_effects=True, vmem_limit_bytes=int(60 * 1024 * 1024)
        ),
    )(
        condition,
        context_condition,
        norm_gain,
        sink,
        jnp.asarray(rot_rows),
        jnp.asarray(rot_cols),
        latent,
        context,
        shift_weight,
        scale_weight,
        gate_weight,
        query_weight,
        key_matrix,
        value_matrix,
        out_weight,
    )


def solution(mesh):
    placed = (
        P(("sp", "tp"), None),
        P("sp"),
        P("sp"),
        P("sp", None),
        P(),
        P("sp", "tp"),
        P("sp", "tp"),
        P("sp", "tp"),
        P(None, "tp"),
        P(None, "tp"),
        P(None, "tp"),
        P("tp"),
        P("tp", None),
    )
    return jax.shard_map(
        functools.partial(shards, mesh.shape["sp"], mesh.shape["tp"]),
        mesh=mesh,
        in_specs=placed,
        out_specs=P(("sp", "tp"), None),
        check_vma=False,
    )
```
